512 devices in a mesh: gr: 2 (over z_hi), sp: 32 (over z_lo, y), tp: 8 (over x, core).
Axes of the slice: x: 4, y: 8, z: 8 (z_hi: 2, z_lo: 4; z = z_hi * 4 + z_lo), core: 2. Of those that a mesh axis runs over, the one named last changes fastest.
Arguments:
- inputs: bfloat16 [16384, 2048], P(('gr', 'sp'), 'tp'), parts along dimension 0, may hold values from -6 to 6
- x_weight: bfloat16 [2048, 4096], P(None, 'tp'), may hold values from -0.125 to 0.125
- b_weight: bfloat16 [2048, 2048], P(None, 'tp'), may hold values from -0.125 to 0.125
- dt_weight: bfloat16 [2048, 128], replicated, may hold values from -0.125 to 0.125
- dt_bias: float32 [2, 64], replicated, may hold values from -2 to -1
- decay_rate: float32 [2, 64], replicated, may hold values from 0.3 to 10
- conv_x: bfloat16 [5, 4096], P(None, 'tp'), may hold values from -2.5 to 2.5
- conv_b: bfloat16 [5, 2048], P(None, 'tp'), may hold values from -2.5 to 2.5
- query_c: bfloat16 [2, 16, 128], P('gr', 'tp'), parts along dimension 0, may hold values from -6 to 6
- query_gate: bfloat16 [2, 64, 64], P('gr', 'tp'), parts along dimension 0, may hold values from -6 to 6
- read_span: int32 [2], P('gr'), parts along dimension 0, may hold values from 0 to 63
- read_gain: float32 [64, 64], P('tp'), may hold values from 0.1 to 1.9
Outputs:
- span_cache: bfloat16 [128, 2, 64, 8192], P('gr', None, 'tp', 'sp'), parts along dimension 0
- first_read: bfloat16 [2, 64, 64], P('gr', 'tp'), parts along dimension 0
The draws below stay inside these ranges and needn't reach their ends.
There are 2 independent parts, one for each index of `gr`. The reference program is written for one: setup_inputs(seed, part) draws one part's arguments, and reference() takes and returns one part's arrays. A program takes and returns all parts, laid end to end along the dimension named above; an argument that names none is the same for every part. Nothing has to cross between parts.
Inputs may be any that keep to these rules, and one draw needn't show every extreme that they name: read_span holds one span index from 0 to 63.
All inputs are finite; a program needn't handle non-finite values.
Results may differ from the reference program's by a relative error of at most 0.009.
Values may be sent and summed in bfloat16 or wider, within the bound.
A program may use at most 64 MiB of HBM per device.

```python
import math
import jax
import jax.numpy as jnp
from jax import lax

D = 2048
H = 64
P_SIZE = 64
G = 16
N = 128
KW = 5
SPAN = 128
LEN = 8192
SPANS = 64


def levels(rng, extent, shards, least, high):
    def one(dim, parts):
        heights = jax.random.uniform(jax.random.fold_in(jax.random.fold_in(rng, 6), dim), (parts,), jnp.float32, least / len(shards), high / len(shards))
        return jnp.repeat(jnp.exp(heights), extent[dim] // parts).reshape((-1,) + (1,) * (len(extent) - dim - 1))

    level = one(*shards[0])
    for cut in shards[1:]:
        level = level * one(*cut)
    return level


def gaussian(rng, extent, width, limit, split=(), kind=jnp.bfloat16):
    entries = jax.random.normal(rng, extent, jnp.float32) * width
    if len(split) > 0:
        entries = levels(rng, extent, split, -0.22, 0.18) * entries
    return jnp.clip(entries, min=-limit, max=limit).astype(kind)


def setup_inputs(seed: int = 0, part: int = 0) -> dict:
    arg_keys = jax.random.split(jax.random.key(seed), 13)
    part_keys = jax.random.split(jax.random.fold_in(arg_keys[12], part), 13)
    return {
        "inputs": gaussian(part_keys[0], (LEN, D), 1.0, 6.0, ((0, 32), (1, 8))),
        "x_weight": gaussian(arg_keys[1], (D, H * P_SIZE), D ** -0.5, 0.125, ((1, 8),)),
        "b_weight": gaussian(arg_keys[2], (D, G * N), D ** -0.5, 0.125, ((1, 8),)),
        "dt_weight": gaussian(arg_keys[3], (D, 2 * H), D ** -0.5, 0.125),
        "dt_bias": jnp.clip(jax.random.uniform(arg_keys[4], (2, H), jnp.float32, -2.0, -1.0), -2.0, -1.0),
        "decay_rate": jnp.clip(jnp.exp(jax.random.uniform(arg_keys[5], (2, H), jnp.float32, math.log(0.3), math.log(10.0))), 0.3, 10.0),
        "conv_x": gaussian(arg_keys[6], (KW, H * P_SIZE), KW ** -0.5, 2.5, ((1, 8),)),
        "conv_b": gaussian(arg_keys[7], (KW, G * N), KW ** -0.5, 2.5, ((1, 8),)),
        "query_c": gaussian(part_keys[8], (1, G, N), 1.0, 6.0, ((1, 8),)),
        "query_gate": gaussian(part_keys[9], (1, H, P_SIZE), 1.0, 6.0, ((1, 8),)),
        "read_span": jax.random.randint(part_keys[10], (1,), 0, SPANS).astype(jnp.int32),
        "read_gain": jnp.clip(1.0 + 0.18 * jax.random.normal(arg_keys[11], (H, P_SIZE), jnp.float32), 0.1, 1.9),
    }


EPSILON = 1e-06

def conv_silu(projected, taps):
    kernel = taps.shape[0]
    reach = kernel // 2
    length = projected.shape[0]
    padded = jnp.pad(projected.astype(jnp.float32), ((reach, reach), (0, 0)))
    result = jnp.zeros((length, projected.shape[1]), jnp.float32)
    for offset in range(kernel):
        result = result + taps[offset].astype(jnp.float32) * padded[offset:offset + length]
    return jax.nn.silu(result).astype(jnp.bfloat16)

def span_states(value_rows, key_rows, step_sizes, log_decay):
    running = jnp.cumsum(log_decay, axis=1)
    closing = running[:, -1]
    forward = jnp.exp(closing[:, None, 0] - running[:, :, 0]) * step_sizes[:, :, 0]
    backward = jnp.exp(running[:, :, 1] - log_decay[:, :, 1]) * step_sizes[:, :, 1]
    weights = jnp.stack([forward, backward], axis=2)
    states = jnp.einsum('kseh,kshn,kshp->kehnp', weights, key_rows.astype(jnp.float32), value_rows.astype(jnp.float32))
    return (states, closing)

def read_weights(span_logs, chosen):
    span_count = span_logs.shape[0]
    ahead_sum = jnp.cumsum(span_logs[:, 0], axis=0)
    behind = jnp.flip(jnp.cumsum(jnp.flip(span_logs[:, 1], 0), axis=0), 0)
    positions = jnp.arange(span_count, dtype=jnp.int32)[:, None]
    ahead_pick = lax.dynamic_slice_in_dim(ahead_sum, chosen, 1, 0)
    behind_pick = lax.dynamic_slice_in_dim(behind, chosen, 1, 0)
    before = positions <= chosen
    after = positions >= chosen
    forward = jnp.where(before, jnp.exp(jnp.where(before, ahead_pick - ahead_sum, 0.0)), 0.0)
    backward = jnp.where(after, jnp.exp(jnp.where(after, behind_pick - behind, 0.0)), 0.0)
    return jnp.stack([forward, backward], axis=1)

def reference(inputs, x_weight, b_weight, dt_weight, dt_bias, decay_rate, conv_x, conv_b, query_c, query_gate, read_span, read_gain):
    length = inputs.shape[0]
    values = conv_silu(jnp.dot(inputs, x_weight, preferred_element_type=jnp.float32).astype(jnp.bfloat16), conv_x)
    key_rows = conv_silu(jnp.dot(inputs, b_weight, preferred_element_type=jnp.float32).astype(jnp.bfloat16), conv_b)
    dt_raw = jnp.dot(inputs, dt_weight, preferred_element_type=jnp.float32).astype(jnp.bfloat16).reshape(length, 2, H)
    step_sizes = jax.nn.softplus(dt_raw.astype(jnp.float32) + dt_bias)
    log_decay = -(step_sizes * decay_rate) / length
    span_count = length // SPAN
    step_sizes = step_sizes.reshape(span_count, SPAN, 2, H)
    log_decay = log_decay.reshape(span_count, SPAN, 2, H)
    span_logs = lax.optimization_barrier(jnp.sum(log_decay, axis=1))
    weights = read_weights(span_logs, read_span[0])
    per_group = H // G

    def one_group(group_index):
        first_head = group_index * per_group
        group_values = lax.dynamic_slice_in_dim(values, first_head * P_SIZE, per_group * P_SIZE, 1).reshape(span_count, SPAN, per_group, P_SIZE)
        group_keys = lax.dynamic_slice_in_dim(key_rows, group_index * N, N, 1).reshape(span_count, SPAN, 1, N)
        group_keys = jnp.broadcast_to(group_keys, (span_count, SPAN, per_group, N))
        group_steps = lax.dynamic_slice_in_dim(step_sizes, first_head, per_group, 3)
        group_logs = lax.dynamic_slice_in_dim(log_decay, first_head, per_group, 3)
        states, unused = span_states(group_values, group_keys, group_steps, group_logs)
        row_block = states.reshape(span_count, 2, per_group, N * P_SIZE).astype(jnp.bfloat16)
        group_weights = lax.dynamic_slice_in_dim(weights, first_head, per_group, 2)
        gathered = jnp.einsum('jeh,jehx->hx', group_weights, row_block.astype(jnp.float32))
        return (row_block, gathered)
    row_block, gathered = lax.map(one_group, jnp.arange(G, dtype=jnp.int32))
    span_cache = jnp.transpose(row_block, (1, 2, 0, 3, 4)).reshape(span_count, 2, H, N * P_SIZE)
    read_state = gathered.reshape(H, N, P_SIZE)
    query_cols = jnp.repeat(query_c[0].astype(jnp.float32), per_group, axis=0)
    read_total = jnp.einsum('hnp,hn->hp', read_state, query_cols)
    gated_read = read_total * jax.nn.silu(query_gate[0].astype(jnp.float32))
    mean_square = jnp.mean(gated_read * gated_read)
    first_read = (gated_read * lax.rsqrt(mean_square + EPSILON) * read_gain)[None].astype(jnp.bfloat16)
    return (span_cache, first_read)
```

```python
import functools
import jax
import jax.numpy as jnp
from jax import lax
from jax.experimental import pallas as pl
from jax.experimental.pallas import tpu as pltpu
from jax.sharding import PartitionSpec as P

H = 64
P_SIZE = 64
G = 16
N = 128
KW = 5
SPAN = 128
EPSILON = 1e-06
LEN = 8192
NY = 8
NZ = 4
NX = 4
NSP = 32
NTP = 8
TOK = 256
FEAT = 256
XC = 512
BC = 256
CC = 768
WC = 896
CH = 2
CROWS = TOK // CH

MESH = pl.DeviceIdType.MESH
F32 = jnp.float32
BF16 = jnp.bfloat16


def iota(shape, dim):
    return lax.broadcasted_iota(jnp.int32, shape, dim)


def kernel(
    inputs, x_weight, b_weight, dt_weight, dt_bias, decay_rate, conv_x, conv_b,
    query_c, query_gate, read_span, read_gain,
    cache, first_read,
    slab, wbuf, acc, proj, mixed, biasb, rateb, cxb, cbb, qb, gateb, gainb, rb,
    closings, expand, sbuf, sendb, ybuf, redy, redz, reds, tot8,
    in_sem, load_sems, gsend, grecv, hsend, hrecv, csend, crecv, asend, arecv,
    ysend, yrecv, zsend, zrecv, ssend, srecv, own_sem, fsem,
):
    sp = lax.axis_index("sp")
    tp = lax.axis_index("tp")
    y = sp % NY
    z = sp // NY
    x = tp // 2
    core = tp % 2
    partner = 2 * x + 1 - core
    right = 2 * ((x + 1) % NX) + core
    left = 2 * ((x + NX - 1) % NX) + core
    across = 2 * ((x + 2) % NX) + core

    own_in = pltpu.make_async_copy(inputs, slab.at[tp], in_sem)
    own_in.start()
    loads = [
        (x_weight, wbuf.at[:, pl.ds(0, XC)]),
        (b_weight, wbuf.at[:, pl.ds(XC, BC)]),
        (dt_weight, wbuf.at[:, pl.ds(CC, 128)]),
        (dt_bias, biasb),
        (decay_rate, rateb),
        (conv_x, cxb),
        (conv_b, cbb),
        (query_c, qb),
        (query_gate, gateb),
        (read_gain, gainb),
        (read_span, rb),
    ]
    copies = []
    for i, (src, dst) in enumerate(loads):
        c = pltpu.make_async_copy(src, dst, load_sems.at[i])
        c.start()
        copies.append(c)

    barrier = pltpu.get_barrier_semaphore()

    def greet_tp(i, carry):
        pl.semaphore_signal(
            barrier, inc=1, device_id={"tp": (tp + i) % NTP}, device_id_type=MESH
        )
        return carry

    def greet_sp(i, carry):
        pl.semaphore_signal(
            barrier, inc=1, device_id={"sp": (sp + i) % NSP}, device_id_type=MESH
        )
        return carry

    lax.fori_loop(1, NTP, greet_tp, 0)
    lax.fori_loop(1, NSP, greet_sp, 0)
    er = iota((256, 1024), 0) % 128
    ec = iota((256, 1024), 1)
    expand[...] = jnp.where(
        er == (ec // 512) * H + tp * 8 + (ec % 512) // P_SIZE, 1.0, 0.0
    ).astype(BF16)
    pl.semaphore_wait(barrier, NTP - 1 + NSP - 1)

    own_in.wait()

    def part(slot, j):
        return slab.at[slot, pl.ds(j * CROWS, CROWS), :]

    sent = []

    def forward(slot, j, dest, index):
        c = pltpu.make_async_remote_copy(
            src_ref=part(slot, j),
            dst_ref=part(slot, j),
            send_sem=gsend.at[index, j],
            recv_sem=grecv.at[slot, j],
            device_id={"tp": dest},
            device_id_type=MESH,
        )
        c.start()
        sent.append(c)

    def arrive(slot, j):
        pltpu.make_async_remote_copy(
            src_ref=part(slot, j),
            dst_ref=part(slot, j),
            send_sem=gsend.at[0, j],
            recv_sem=grecv.at[slot, j],
            device_id={"tp": partner},
            device_id_type=MESH,
        ).wait_recv()

    for j in range(CH):
        forward(tp, j, right, 0)
        forward(tp, j, left, 1)
        forward(tp, j, partner, 2)

    for c in copies:
        c.wait()

    def product(slot):
        rows = pl.ds(pl.multiple_of(slot * FEAT, FEAT), FEAT)
        return jnp.dot(slab[slot], wbuf[rows, :], preferred_element_type=F32)

    fwd_slot = left * (1 - core) + right * core
    oth_slot = right * (1 - core) + left * core
    fwd_dest = oth_slot
    acc[...] = product(tp)
    for j in range(CH):
        arrive(fwd_slot, j)
        forward(fwd_slot, j, fwd_dest, 3)
        forward(fwd_slot, j, partner, 4)
        arrive(oth_slot, j)
        forward(oth_slot, j, partner, 5)
    for j in range(CH):
        arrive(partner, j)
    acc[...] += product(partner)
    acc[...] += product(fwd_slot)
    acc[...] += product(oth_slot)
    for j in range(CH):
        arrive(across, j)
        forward(across, j, partner, 6)
    acc[...] += product(across)
    for other in (left, right):
        peer = other + 1 - 2 * core
        for j in range(CH):
            arrive(peer, j)
        acc[...] += product(peer)
    peer = across + 1 - 2 * core
    for j in range(CH):
        arrive(peer, j)
    last = product(peer)
    proj[pl.ds(8, TOK), :] = (acc[:, :CC] + last[:, :CC]).astype(BF16).astype(F32)
    dt_raw = (acc[:, CC:] + last[:, CC:]).astype(BF16).astype(F32)

    def edge_up():
        return pltpu.make_async_remote_copy(
            src_ref=proj.at[pl.ds(TOK, 8), :],
            dst_ref=proj.at[pl.ds(0, 8), :],
            send_sem=hsend.at[0],
            recv_sem=hrecv.at[0],
            device_id={"sp": (sp + 1) % NSP},
            device_id_type=MESH,
        )

    def edge_down():
        return pltpu.make_async_remote_copy(
            src_ref=proj.at[pl.ds(8, 8), :],
            dst_ref=proj.at[pl.ds(TOK + 8, 8), :],
            send_sem=hsend.at[1],
            recv_sem=hrecv.at[1],
            device_id={"sp": (sp + NSP - 1) % NSP},
            device_id_type=MESH,
        )

    edge_up().start()
    edge_down().start()

    bias = jnp.concatenate([biasb[0:1, :], biasb[1:2, :]], axis=1)
    rate = jnp.concatenate([rateb[0:1, :], rateb[1:2, :]], axis=1)
    v = dt_raw + bias
    step = jnp.maximum(v, 0.0) + jnp.log1p(jnp.exp(-jnp.abs(v)))
    decay = -(step * rate) / LEN
    row = iota((SPAN, SPAN), 0)
    col = iota((SPAN, SPAN), 1)
    later = jnp.where(col > row, 1.0, 0.0)
    earlier = jnp.where(col < row, 1.0, 0.0)
    ws = []
    for k in range(2):
        a = decay[k * SPAN : (k + 1) * SPAN]
        tail = jnp.dot(later, a, precision=lax.Precision.HIGHEST, preferred_element_type=F32)
        head = jnp.dot(earlier, a, precision=lax.Precision.HIGHEST, preferred_element_type=F32)
        w = jnp.exp(jnp.where(col < H, tail, head)) * step[k * SPAN : (k + 1) * SPAN]
        closings[sp, k : k + 1, :] = jnp.sum(a, axis=0, keepdims=True)
        ws.append(w)

    def closing_copy(d, s):
        return pltpu.make_async_remote_copy(
            src_ref=closings.at[s],
            dst_ref=closings.at[s],
            send_sem=csend.at[d],
            recv_sem=crecv.at[s],
            device_id={"sp": d},
            device_id_type=MESH,
        )

    def send_closing(i, carry):
        closing_copy((sp + i) % NSP, sp).start()
        return carry

    lax.fori_loop(1, NSP, send_closing, 0)

    w = jnp.concatenate(ws, axis=0)
    w_high = w.astype(BF16)
    w_low = (w - w_high.astype(F32)).astype(BF16)
    pair = jnp.concatenate([w_high, w_low], axis=1)

    taps = [cxb[...].astype(F32), cbb[...].astype(F32)]

    def convolve(start, count):
        for block in range(CC // 256):
            tap = taps[0][:, block * 256 : (block + 1) * 256] if block < 2 else taps[1]
            cols = pl.ds(block * 256, 256)
            total = jnp.zeros((count, 256), F32)
            for o in range(KW):
                total = total + tap[o : o + 1] * proj[pl.ds(start + 6 + o, count), cols]
            mixed[pl.ds(start, count), cols] = jax.nn.silu(total).astype(BF16)

    for start in range(16, TOK - 16, 32):
        convolve(start, 32)

    edge_up().wait_recv()
    edge_down().wait_recv()

    @pl.when(sp == 0)
    def _():
        proj[pl.ds(0, 8), :] = jnp.zeros((8, CC), F32)

    @pl.when(sp == NSP - 1)
    def _():
        proj[pl.ds(TOK + 8, 8), :] = jnp.zeros((8, CC), F32)

    convolve(0, 16)
    convolve(TOK - 16, 16)

    order = (4 * (row % 32) + row // 32 == col)
    order_t = jnp.where(order, 1.0, 0.0).astype(BF16)
    contract_last = (((1,), (1,)), ((), ()))
    queries = []
    for g in range(2):
        q8 = jnp.broadcast_to(qb[0, g : g + 1, :].astype(F32), (8, N)).astype(BF16)
        queries.append(
            lax.dot_general(q8, order_t, contract_last, preferred_element_type=F32).astype(BF16)
        )
    half = iota((32, 128), 1) < P_SIZE

    def state_copy(d, s):
        return pltpu.make_async_remote_copy(
            src_ref=sendb.at[d],
            dst_ref=cache.at[pl.ds(2 * s, 2)],
            send_sem=asend.at[d],
            recv_sem=arecv.at[s],
            device_id={"sp": d},
            device_id_type=MESH,
        )

    for k in range(2):
        rows = pl.ds(k * SPAN, SPAN)
        keys_t = [
            lax.dot_general(
                order_t, mixed[rows, pl.ds(XC + g * N, N)], contract_last,
                preferred_element_type=F32,
            ).astype(BF16)
            for g in range(2)
        ]
        for e in range(2):
            wide = jnp.dot(
                pair[k * SPAN : (k + 1) * SPAN],
                expand[:, pl.ds(e * 512, 512)],
                preferred_element_type=F32,
            )
            weighted = (mixed[rows, pl.ds(0, XC)].astype(F32) * wide).astype(BF16)
            for g in range(2):
                state = jnp.dot(
                    keys_t[g], weighted[:, g * 256 : (g + 1) * 256], preferred_element_type=F32
                )
                rounded = state.astype(BF16)
                read = jnp.dot(queries[g], rounded, preferred_element_type=F32)
                ybuf[2 * k + e : 2 * k + e + 1, pl.ds(g * 256, 256)] = read[0:1]
                for j in range(2):
                    for a in range(2):
                        one = state[64 * a : 64 * a + 32, 128 * j : 128 * j + 128]
                        two = state[64 * a + 32 : 64 * a + 64, 128 * j : 128 * j + 128]
                        first = jnp.where(half, one, pltpu.roll(two, 64, 1))
                        second = jnp.where(half, pltpu.roll(one, 64, 1), two)
                        h = 4 * g + 2 * j
                        sbuf[a, pl.ds(h, 32, stride=8), :] = first
                        sbuf[a, pl.ds(h + 1, 32, stride=8), :] = second
            for a in range(2):
                sendb[:, k, e, :, pl.ds(a * 128, 128)] = sbuf[a].reshape(NSP, 8, 128).astype(BF16)

    own_out = pltpu.make_async_copy(sendb.at[sp], cache.at[pl.ds(2 * sp, 2)], own_sem)
    own_out.start()

    def peer_at(i):
        m = 7 - i % 8
        dy = (m % 2) * ((m + 1) // 2) + (1 - m % 2) * ((8 - m // 2) % 8)
        dz = 3 - i // 8
        return ((z + dz) % NZ) * NY + (y + dy) % NY

    def send_state(i, carry):
        state_copy(peer_at(i), sp).start()
        return carry

    lax.fori_loop(0, NSP - 1, send_state, 0)

    def closing_arrives(i, carry):
        s = (sp + i) % NSP
        closing_copy(s, s).wait_recv()
        return carry

    lax.fori_loop(1, NSP, closing_arrives, 0)
    chosen = rb[0]
    shape = (NSP, 2, 128)
    logs = closings[...]
    where_at = 2 * iota(shape, 0) + iota(shape, 1)
    forward_lane = iota(shape, 2) < H
    lane = iota((1, 128), 1)
    factors = []
    for k in range(2):
        mine = 2 * sp + k
        ahead = jnp.where(where_at > mine, jnp.where(where_at <= chosen, 1.0, 0.0), 0.0)
        behind = jnp.where(where_at >= chosen, jnp.where(where_at < mine, 1.0, 0.0), 0.0)
        picked = logs * jnp.where(forward_lane, ahead, behind)
        log_sum = jnp.sum(jnp.sum(picked, axis=0), axis=0, keepdims=True)
        at = jnp.full((1, 128), mine, jnp.int32)
        pick = jnp.full((1, 128), chosen, jnp.int32)
        live = jnp.where(
            lane < H,
            jnp.where(at <= pick, 1.0, 0.0),
            jnp.where(at >= pick, 1.0, 0.0),
        )
        factors.append(jnp.exp(log_sum) * live)
    factor = jnp.concatenate([jnp.broadcast_to(f, (8, 128)) for f in factors], axis=0)
    f_high = factor.astype(BF16)
    f_low = (factor - f_high.astype(F32)).astype(BF16)
    spread = jnp.dot(
        jnp.concatenate([f_high, f_low], axis=1), expand[...], preferred_element_type=F32
    )
    partial = jnp.zeros((1, 512), F32)
    for k in range(2):
        for e in range(2):
            partial = partial + (
                spread[8 * k : 8 * k + 1, e * 512 : (e + 1) * 512]
                * ybuf[2 * k + e : 2 * k + e + 1, :]
            )
    for i in range(4):
        redy[y, i : i + 1, :] = partial[:, i * 128 : (i + 1) * 128]

    def y_copy(d, s):
        return pltpu.make_async_remote_copy(
            src_ref=redy.at[s],
            dst_ref=redy.at[s],
            send_sem=ysend.at[d],
            recv_sem=yrecv.at[s],
            device_id={"sp": z * NY + d},
            device_id_type=MESH,
        )

    def z_copy(d, s):
        return pltpu.make_async_remote_copy(
            src_ref=redz.at[s],
            dst_ref=redz.at[s],
            send_sem=zsend.at[d],
            recv_sem=zrecv.at[s],
            device_id={"sp": d * NY + y},
            device_id_type=MESH,
        )

    def s_copy(d, s):
        return pltpu.make_async_remote_copy(
            src_ref=reds.at[s],
            dst_ref=reds.at[s],
            send_sem=ssend.at[d],
            recv_sem=srecv.at[s],
            device_id={"tp": d},
            device_id_type=MESH,
        )

    def each(copy, me, count, act):
        def body(i, carry):
            act(copy, me, (me + i) % count)
            return carry

        lax.fori_loop(1, count, body, 0)

    def start(copy, me, other):
        copy(other, me).start()

    def receive(copy, me, other):
        copy(other, other).wait_recv()

    def leave(copy, me, other):
        copy(other, me).wait_send()

    each(y_copy, y, NY, start)
    each(y_copy, y, NY, receive)
    redz[z] = jnp.sum(redy[...], axis=0)
    each(z_copy, z, NZ, start)
    each(z_copy, z, NZ, receive)
    total = jnp.sum(redz[...], axis=0)
    for h in range(8):
        tot8[h : h + 1, :] = total[h // 2 : h // 2 + 1, (h % 2) * 64 : (h % 2) * 64 + 64]
    gated = tot8[...] * jax.nn.silu(gateb[0].astype(F32))
    squares = jnp.sum(jnp.sum(gated * gated, axis=0, keepdims=True), axis=1, keepdims=True)
    reds[tp] = jnp.broadcast_to(squares, (1, 128))
    each(s_copy, tp, NTP, start)
    each(s_copy, tp, NTP, receive)
    square_sum = jnp.sum(reds[...], axis=0)[:, :64]
    scale = lax.rsqrt(square_sum / (H * P_SIZE) + EPSILON)
    tot8[...] = gated * scale * gainb[...]
    gateb[0] = tot8[...].astype(BF16)
    final = pltpu.make_async_copy(gateb, first_read, fsem)
    final.start()

    def state_arrives(i, carry):
        s = (sp + i) % NSP
        state_copy(s, s).wait_recv()
        return carry

    for c in sent:
        c.wait_send()
    edge_up().wait_send()
    edge_down().wait_send()
    each(closing_copy, sp, NSP, leave)
    each(y_copy, y, NY, leave)
    each(z_copy, z, NZ, leave)
    each(s_copy, tp, NTP, leave)
    lax.fori_loop(1, NSP, state_arrives, 0)
    each(state_copy, sp, NSP, leave)
    own_out.wait()
    final.wait()


def per_device(*args):
    dma = pltpu.SemaphoreType.DMA
    any_spec = pl.BlockSpec(memory_space=pl.ANY)
    return pl.pallas_call(
        kernel,
        out_shape=(
            jax.ShapeDtypeStruct((64, 2, 8, 256), BF16),
            jax.ShapeDtypeStruct((1, 8, 64), BF16),
        ),
        in_specs=[any_spec] * 12,
        out_specs=(any_spec, any_spec),
        scratch_shapes=[
            pltpu.VMEM((NTP, TOK, FEAT), BF16),
            pltpu.VMEM((2048, WC), BF16),
            pltpu.VMEM((TOK, WC), F32),
            pltpu.VMEM((TOK + 16, CC), F32),
            pltpu.VMEM((TOK, CC), BF16),
            pltpu.VMEM((2, H), F32),
            pltpu.VMEM((2, H), F32),
            pltpu.VMEM((KW, XC), BF16),
            pltpu.VMEM((KW, BC), BF16),
            pltpu.VMEM((1, 2, N), BF16),
            pltpu.VMEM((1, 8, P_SIZE), BF16),
            pltpu.VMEM((8, P_SIZE), F32),
            pltpu.SMEM((1,), jnp.int32),
            pltpu.VMEM((NSP, 2, 128), F32),
            pltpu.VMEM((256, 1024), BF16),
            pltpu.VMEM((2, 256, 128), F32),
            pltpu.VMEM((NSP, 2, 2, 8, 256), BF16),
            pltpu.VMEM((8, 512), F32),
            pltpu.VMEM((NY, 4, 128), F32),
            pltpu.VMEM((NZ, 4, 128), F32),
            pltpu.VMEM((NTP, 1, 128), F32),
            pltpu.VMEM((8, P_SIZE), F32),
            dma,
            dma((11,)),
            dma((7, CH)),
            dma((NTP, CH)),
            dma((2,)),
            dma((2,)),
            dma((NSP,)),
            dma((NSP,)),
            dma((NSP,)),
            dma((NSP,)),
            dma((NY,)),
            dma((NY,)),
            dma((NZ,)),
            dma((NZ,)),
            dma((NTP,)),
            dma((NTP,)),
            dma,
            dma,
        ],
        compiler_params=pltpu.CompilerParams(collective_id=0, has_side_effects=True),
    )(*args)


def solution(mesh):
    return jax.shard_map(
        per_device,
        mesh=mesh,
        in_specs=(
            P(("gr", "sp"), "tp"),
            P(None, "tp"),
            P(None, "tp"),
            P(),
            P(),
            P(),
            P(None, "tp"),
            P(None, "tp"),
            P("gr", "tp", None),
            P("gr", "tp", None),
            P("gr"),
            P("tp", None),
        ),
        out_specs=(P("gr", None, "tp", "sp"), P("gr", "tp", None)),
        check_vma=False,
    )
```

```python
import functools
import jax
import jax.numpy as jnp
from jax import lax
from jax.experimental import pallas as pl
from jax.experimental.pallas import tpu as pltpu
from jax.sharding import PartitionSpec as P

H = 64
P_SIZE = 64
G = 16
N = 128
KW = 5
SPAN = 128
EPSILON = 1e-06
LEN = 8192
NY = 8
NZ = 4
NX = 4
NSP = 32
NTP = 8
TOK = 256
FEAT = 256
XC = 512
BC = 256
CC = 768
WC = 896
CH = 4
EARLY = 3
CROWS = TOK // CH

MESH = pl.DeviceIdType.MESH
F32 = jnp.float32
BF16 = jnp.bfloat16


def iota(shape, dim):
    return lax.broadcasted_iota(jnp.int32, shape, dim)


def kernel(
    inputs, x_weight, b_weight, dt_weight, dt_bias, decay_rate, conv_x, conv_b,
    query_c, query_gate, read_span, read_gain,
    cache, first_read,
    slab, wbuf, acc, proj, mixed, biasb, rateb, cxb, cbb, qb, gateb, gainb, rb,
    closings, blocks, expand, sbuf, sendb, ybuf, redy, redz, reds, tot8,
    in_sem, load_sems, gsend, grecv, hsend, hrecv, csend, crecv, asend, arecv,
    ysend, yrecv, zsend, zrecv, usend, urecv, ssend, srecv, own_sem, stage,
):
    sp = lax.axis_index("sp")
    tp = lax.axis_index("tp")
    y = sp % NY
    z = sp // NY
    x = tp // 2
    core = tp % 2
    partner = 2 * x + 1 - core
    right = 2 * ((x + 1) % NX) + core
    left = 2 * ((x + NX - 1) % NX) + core
    across = 2 * ((x + 2) % NX) + core

    own_in = pltpu.make_async_copy(inputs, slab.at[tp], in_sem)
    own_in.start()
    loads = [
        (x_weight, wbuf.at[:, pl.ds(0, XC)]),
        (b_weight, wbuf.at[:, pl.ds(XC, BC)]),
        (dt_weight, wbuf.at[:, pl.ds(CC, 128)]),
        (dt_bias, biasb),
        (decay_rate, rateb),
        (conv_x, cxb),
        (conv_b, cbb),
        (query_c, qb),
        (query_gate, gateb),
        (read_gain, gainb),
        (read_span, rb),
    ]
    copies = []
    for i, (src, dst) in enumerate(loads):
        c = pltpu.make_async_copy(src, dst, load_sems.at[i])
        c.start()
        copies.append(c)

    barrier = pltpu.get_barrier_semaphore()

    def at_y(other):
        return {"sp": z * NY + (other + NY) % NY}

    def greet_tp(i, carry):
        pl.semaphore_signal(
            barrier, inc=1, device_id={"tp": (tp + i) % NTP}, device_id_type=MESH
        )
        return carry

    def greet_z(i, carry):
        pl.semaphore_signal(
            barrier, inc=1, device_id={"sp": ((z + i) % NZ) * NY + y}, device_id_type=MESH
        )
        return carry

    lax.fori_loop(1, NTP, greet_tp, 0)
    lax.fori_loop(1, NZ, greet_z, 0)
    for side in (1, -1):
        pl.semaphore_signal(barrier, inc=1, device_id=at_y(y + side), device_id_type=MESH)

    def tell(index, distance):
        for side in (distance, -distance):
            pl.semaphore_signal(
                stage.at[index], inc=1, device_id=at_y(y + side), device_id_type=MESH
            )

    er = iota((256, 1024), 0) % 128
    ec = iota((256, 1024), 1)
    expand[...] = jnp.where(
        er == (ec // 512) * H + tp * 8 + (ec % 512) // P_SIZE, 1.0, 0.0
    ).astype(BF16)
    pl.semaphore_wait(barrier, NTP - 1 + NZ - 1 + 2)
    tell(0, 1)

    own_in.wait()

    def part(slot, j):
        return slab.at[slot, pl.ds(j * CROWS, CROWS), :]

    sent = []

    def forward(slot, j, dest, index):
        c = pltpu.make_async_remote_copy(
            src_ref=part(slot, j),
            dst_ref=part(slot, j),
            send_sem=gsend.at[index, j],
            recv_sem=grecv.at[slot, j],
            device_id={"tp": dest},
            device_id_type=MESH,
        )
        c.start()
        sent.append(c)

    def arrive(slot, j):
        pltpu.make_async_remote_copy(
            src_ref=part(slot, j),
            dst_ref=part(slot, j),
            send_sem=gsend.at[0, j],
            recv_sem=grecv.at[slot, j],
            device_id={"tp": partner},
            device_id_type=MESH,
        ).wait_recv()

    for j in range(CH):
        forward(tp, j, right, 0)
        forward(tp, j, left, 1)
    for j in range(CH):
        forward(tp, j, partner, 2)

    for c in copies:
        c.wait()

    def product(slot):
        rows = pl.ds(pl.multiple_of(slot * FEAT, FEAT), FEAT)
        return jnp.dot(slab[slot], wbuf[rows, :], preferred_element_type=F32)

    fwd_slot = left * (1 - core) + right * core
    oth_slot = right * (1 - core) + left * core
    fwd_dest = oth_slot
    acc[...] = product(tp)
    for j in range(CH):
        arrive(fwd_slot, j)
        forward(fwd_slot, j, fwd_dest, 3)
        forward(fwd_slot, j, partner, 4)
        arrive(oth_slot, j)
        forward(oth_slot, j, partner, 5)
        if j == 0:
            for i in range(CH):
                arrive(partner, i)
            acc[...] += product(partner)
            pl.semaphore_wait(stage.at[0], 2)
            tell(1, 2)
    acc[...] += product(fwd_slot)
    pl.semaphore_wait(stage.at[1], 2)
    tell(2, 1)
    acc[...] += product(oth_slot)
    others = [left + 1 - 2 * core, right + 1 - 2 * core]
    for j in range(CH):
        arrive(across, j)
        forward(across, j, partner, 6)
        if j % 2 == 1:
            peer = others[j // 2]
            for i in range(CH):
                arrive(peer, i)
            acc[...] += product(peer)
    acc[...] += product(across)
    peer = across + 1 - 2 * core
    for j in range(CH):
        arrive(peer, j)
    last = product(peer)
    pl.semaphore_wait(stage.at[2], 2)
    proj[pl.ds(8, TOK), :] = (acc[:, :CC] + last[:, :CC]).astype(BF16).astype(F32)
    dt_raw = (acc[:, CC:] + last[:, CC:]).astype(BF16).astype(F32)

    def edge_up():
        return pltpu.make_async_remote_copy(
            src_ref=proj.at[pl.ds(TOK, 8), :],
            dst_ref=proj.at[pl.ds(0, 8), :],
            send_sem=hsend.at[0],
            recv_sem=hrecv.at[0],
            device_id={"sp": (sp + 1) % NSP},
            device_id_type=MESH,
        )

    def edge_down():
        return pltpu.make_async_remote_copy(
            src_ref=proj.at[pl.ds(8, 8), :],
            dst_ref=proj.at[pl.ds(TOK + 8, 8), :],
            send_sem=hsend.at[1],
            recv_sem=hrecv.at[1],
            device_id={"sp": (sp + NSP - 1) % NSP},
            device_id_type=MESH,
        )

    edge_up().start()
    edge_down().start()

    bias = jnp.concatenate([biasb[0:1, :], biasb[1:2, :]], axis=1)
    rate = jnp.concatenate([rateb[0:1, :], rateb[1:2, :]], axis=1)
    v = dt_raw + bias
    step = jnp.maximum(v, 0.0) + jnp.log1p(jnp.exp(-jnp.abs(v)))
    decay = -(step * rate) / LEN
    row = iota((SPAN, SPAN), 0)
    col = iota((SPAN, SPAN), 1)
    later = jnp.where(col > row, 1.0, 0.0)
    earlier = jnp.where(col < row, 1.0, 0.0)
    ws = []
    for k in range(2):
        a = decay[k * SPAN : (k + 1) * SPAN]
        tail = jnp.dot(later, a, precision=lax.Precision.HIGHEST, preferred_element_type=F32)
        head = jnp.dot(earlier, a, precision=lax.Precision.HIGHEST, preferred_element_type=F32)
        w = jnp.exp(jnp.where(col < H, tail, head)) * step[k * SPAN : (k + 1) * SPAN]
        closings[y, k : k + 1, :] = jnp.sum(a, axis=0, keepdims=True)
        ws.append(w)

    def y_exchange(buffer, send_sem, recv_sem):
        return lambda d, s: pltpu.make_async_remote_copy(
            src_ref=buffer.at[s],
            dst_ref=buffer.at[s],
            send_sem=send_sem.at[d],
            recv_sem=recv_sem.at[s],
            device_id=at_y(d),
            device_id_type=MESH,
        )

    def z_exchange(buffer, send_sem, recv_sem):
        return lambda d, s: pltpu.make_async_remote_copy(
            src_ref=buffer.at[s],
            dst_ref=buffer.at[s],
            send_sem=send_sem.at[d],
            recv_sem=recv_sem.at[s],
            device_id={"sp": d * NY + y},
            device_id_type=MESH,
        )

    closing_copy = y_exchange(closings, csend, crecv)
    y_copy = y_exchange(redy, ysend, yrecv)
    z_copy = z_exchange(redz, zsend, zrecv)
    block_copy = z_exchange(blocks, usend, urecv)

    def each(copy, me, count, act):
        def body(i, carry):
            act(copy, me, (me + i) % count)
            return carry

        lax.fori_loop(1, count, body, 0)

    def start(copy, me, other):
        copy(other, me).start()

    def receive(copy, me, other):
        copy(other, other).wait_recv()

    def leave(copy, me, other):
        copy(other, me).wait_send()

    each(closing_copy, y, NY, start)

    w = jnp.concatenate(ws, axis=0)
    w_high = w.astype(BF16)
    w_low = (w - w_high.astype(F32)).astype(BF16)
    pair = jnp.concatenate([w_high, w_low], axis=1)

    taps = [cxb[...].astype(F32), cbb[...].astype(F32)]

    def convolve(start, count):
        for block in range(CC // 256):
            tap = taps[0][:, block * 256 : (block + 1) * 256] if block < 2 else taps[1]
            cols = pl.ds(block * 256, 256)
            total = jnp.zeros((count, 256), F32)
            for o in range(KW):
                total = total + tap[o : o + 1] * proj[pl.ds(start + 6 + o, count), cols]
            mixed[pl.ds(start, count), cols] = jax.nn.silu(total).astype(BF16)

    order = (4 * (row % 32) + row // 32 == col)
    order_t = jnp.where(order, 1.0, 0.0).astype(BF16)
    contract_last = (((1,), (1,)), ((), ()))
    queries = []
    for g in range(2):
        q8 = jnp.broadcast_to(qb[0, g : g + 1, :].astype(F32), (8, N)).astype(BF16)
        queries.append(
            lax.dot_general(q8, order_t, contract_last, preferred_element_type=F32).astype(BF16)
        )
    half = iota((32, 128), 1) < P_SIZE

    def state_copy(k, d, s):
        return pltpu.make_async_remote_copy(
            src_ref=sendb.at[d, k],
            dst_ref=cache.at[2 * s + k],
            send_sem=asend.at[k, d],
            recv_sem=arecv.at[k, s],
            device_id={"sp": d},
            device_id_type=MESH,
        )

    def send_states(k, first, last):
        def body(i, carry):
            m = 7 - (first + i // NZ)
            dy = (m % 2) * ((m + 1) // 2) + (1 - m % 2) * (8 - m // 2)
            d = ((z + i % NZ) % NZ) * NY + (y + dy) % NY
            state_copy(k, d, sp).start()
            return carry

        lax.fori_loop(0, (last - first) * NZ, body, 0)

    def send_column(k):
        def body(i, carry):
            state_copy(k, ((z + i) % NZ) * NY + y, sp).start()
            return carry

        lax.fori_loop(1, NZ, body, 0)

    own_out = []
    for k in range(2):
        rows = pl.ds(k * SPAN, SPAN)
        if k == 0:
            for first in range(16, SPAN, 16):
                convolve(first, 16)
            edge_up().wait_recv()

            @pl.when(sp == 0)
            def _():
                proj[pl.ds(0, 8), :] = jnp.zeros((8, CC), F32)

            convolve(0, 16)
        else:
            for first in range(SPAN, TOK - 16, 16):
                convolve(first, 16)
            edge_down().wait_recv()

            @pl.when(sp == NSP - 1)
            def _():
                proj[pl.ds(TOK + 8, 8), :] = jnp.zeros((8, CC), F32)

            convolve(TOK - 16, 16)
        keys_t = [
            lax.dot_general(
                order_t, mixed[rows, pl.ds(XC + g * N, N)], contract_last,
                preferred_element_type=F32,
            ).astype(BF16)
            for g in range(2)
        ]
        for e in range(2):
            wide = jnp.dot(
                pair[k * SPAN : (k + 1) * SPAN],
                expand[:, pl.ds(e * 512, 512)],
                preferred_element_type=F32,
            )
            weighted = (mixed[rows, pl.ds(0, XC)].astype(F32) * wide).astype(BF16)
            for g in range(2):
                state = jnp.dot(
                    keys_t[g], weighted[:, g * 256 : (g + 1) * 256], preferred_element_type=F32
                )
                rounded = state.astype(BF16)
                read = jnp.dot(queries[g], rounded, preferred_element_type=F32)
                ybuf[k : k + 1, pl.ds(e * 512 + g * 256, 256)] = read[0:1]
                for j in range(2):
                    for a in range(2):
                        one = state[64 * a : 64 * a + 32, 128 * j : 128 * j + 128]
                        two = state[64 * a + 32 : 64 * a + 64, 128 * j : 128 * j + 128]
                        first = jnp.where(half, one, pltpu.roll(two, 64, 1))
                        second = jnp.where(half, pltpu.roll(one, 64, 1), two)
                        h = 4 * g + 2 * j
                        sbuf[a, pl.ds(h, 32, stride=8), :] = first
                        sbuf[a, pl.ds(h + 1, 32, stride=8), :] = second
            for a in range(2):
                sendb[:, k, e, :, pl.ds(a * 128, 128)] = sbuf[a].reshape(NSP, 8, 128).astype(BF16)

        own_out.append(
            pltpu.make_async_copy(sendb.at[sp, k], cache.at[2 * sp + k], own_sem.at[k])
        )
        own_out[k].start()
        if k == 0:
            send_column(0)
            send_states(0, 0, EARLY)

    each(closing_copy, y, NY, receive)
    chosen = rb[0]
    shape = (NY, 2, 128)
    logs = closings[...]
    where_at = 2 * NY * z + 2 * iota(shape, 0) + iota(shape, 1)
    forward_lane = iota(shape, 2) < H
    up_to = jnp.where(where_at <= chosen, 1.0, 0.0)
    on_from = jnp.where(where_at >= chosen, 1.0, 0.0)
    lane = iota((1, 128), 1)

    def log_total(ahead, behind):
        picked = logs * jnp.where(forward_lane, ahead, behind)
        return jnp.sum(jnp.sum(picked, axis=0), axis=0, keepdims=True)

    blocks[z] = log_total(up_to, on_from)
    each(block_copy, z, NZ, start)
    factors = []
    for k in range(2):
        mine = 2 * sp + k
        log_sum = log_total(
            jnp.where(where_at > mine, up_to, 0.0), jnp.where(where_at < mine, on_from, 0.0)
        )
        at = jnp.full((1, 128), mine, jnp.int32)
        pick = jnp.full((1, 128), chosen, jnp.int32)
        live = jnp.where(
            lane < H,
            jnp.where(at <= pick, 1.0, 0.0),
            jnp.where(at >= pick, 1.0, 0.0),
        )
        factors.append(jnp.broadcast_to(jnp.exp(log_sum) * live, (8, 128)))

    def spread(rows):
        high = rows.astype(BF16)
        low = (rows - high.astype(F32)).astype(BF16)
        return jnp.dot(
            jnp.concatenate([high, low], axis=1), expand[...], preferred_element_type=F32
        )

    wide_factor = spread(jnp.concatenate(factors, axis=0))
    redy[y] = wide_factor[0:1] * ybuf[0:1, :] + wide_factor[8:9] * ybuf[1:2, :]
    each(y_copy, y, NY, start)
    send_states(0, EARLY, 7)
    send_column(1)
    send_states(1, 0, 7)

    each(block_copy, z, NZ, receive)
    block_rows = []
    for block in range(NZ):
        after = jnp.zeros((1, 128), F32)
        before = jnp.zeros((1, 128), F32)
        for other in range(block + 1, NZ):
            after = after + blocks[other]
        for other in range(block):
            before = before + blocks[other]
        block_rows.append(
            jnp.broadcast_to(jnp.exp(jnp.where(lane < H, after, before)), (8, 128))
        )
    block_factor = spread(jnp.concatenate(block_rows, axis=0))
    gate = jax.nn.silu(gateb[0].astype(F32))

    def s_copy(d, s):
        return pltpu.make_async_remote_copy(
            src_ref=reds.at[s],
            dst_ref=reds.at[s],
            send_sem=ssend.at[d],
            recv_sem=srecv.at[s],
            device_id={"tp": d},
            device_id_type=MESH,
        )

    each(y_copy, y, NY, receive)
    redz[z] = jnp.sum(redy[...], axis=0)
    each(z_copy, z, NZ, start)
    each(z_copy, z, NZ, receive)
    both = jnp.zeros((1, 1024), F32)
    for block in range(NZ):
        both = both + block_factor[8 * block : 8 * block + 1] * redz[block]
    total = both[:, :512] + both[:, 512:]
    for h in range(8):
        tot8[h : h + 1, :] = total[:, h * P_SIZE : (h + 1) * P_SIZE]
    gated = tot8[...] * gate
    squares = jnp.sum(jnp.sum(gated * gated, axis=0, keepdims=True), axis=1, keepdims=True)
    reds[tp] = jnp.broadcast_to(squares, (1, 128))
    each(s_copy, tp, NTP, start)
    each(s_copy, tp, NTP, receive)
    square_sum = jnp.sum(reds[...], axis=0)[:, :64]
    scale = lax.rsqrt(square_sum / (H * P_SIZE) + EPSILON)
    first_read[0] = (gated * scale * gainb[...]).astype(BF16)

    for c in sent:
        c.wait_send()
    edge_up().wait_send()
    edge_down().wait_send()
    each(closing_copy, y, NY, leave)
    each(block_copy, z, NZ, leave)
    each(y_copy, y, NY, leave)
    each(z_copy, z, NZ, leave)
    each(s_copy, tp, NTP, leave)
    for k in range(2):
        each(functools.partial(state_copy, k), sp, NSP, receive)
        each(functools.partial(state_copy, k), sp, NSP, leave)
        own_out[k].wait()


def per_device(*args):
    dma = pltpu.SemaphoreType.DMA
    any_spec = pl.BlockSpec(memory_space=pl.ANY)
    vmem_spec = pl.BlockSpec(memory_space=pltpu.VMEM)
    shapes = (
        jax.ShapeDtypeStruct((64, 2, 8, 256), BF16),
        jax.ShapeDtypeStruct((1, 8, 64), BF16),
    )
    return pl.pallas_call(
        kernel,
        out_shape=tuple(pltpu.VMEM(t.shape, t.dtype) for t in shapes),
        in_specs=[any_spec] * 12,
        out_specs=(vmem_spec, vmem_spec),
        scratch_shapes=[
            pltpu.VMEM((NTP, TOK, FEAT), BF16),
            pltpu.VMEM((2048, WC), BF16),
            pltpu.VMEM((TOK, WC), F32),
            pltpu.VMEM((TOK + 16, CC), F32),
            pltpu.VMEM((TOK, CC), BF16),
            pltpu.VMEM((2, H), F32),
            pltpu.VMEM((2, H), F32),
            pltpu.VMEM((KW, XC), BF16),
            pltpu.VMEM((KW, BC), BF16),
            pltpu.VMEM((1, 2, N), BF16),
            pltpu.VMEM((1, 8, P_SIZE), BF16),
            pltpu.VMEM((8, P_SIZE), F32),
            pltpu.SMEM((1,), jnp.int32),
            pltpu.VMEM((NY, 2, 128), F32),
            pltpu.VMEM((NZ, 1, 128), F32),
            pltpu.VMEM((256, 1024), BF16),
            pltpu.VMEM((2, 256, 128), F32),
            pltpu.VMEM((NSP, 2, 2, 8, 256), BF16),
            pltpu.VMEM((8, 1024), F32),
            pltpu.VMEM((NY, 1, 1024), F32),
            pltpu.VMEM((NZ, 1, 1024), F32),
            pltpu.VMEM((NTP, 1, 128), F32),
            pltpu.VMEM((8, P_SIZE), F32),
            dma,
            dma((11,)),
            dma((7, CH)),
            dma((NTP, CH)),
            dma((2,)),
            dma((2,)),
            dma((NY,)),
            dma((NY,)),
            dma((2, NSP)),
            dma((2, NSP)),
            dma((NY,)),
            dma((NY,)),
            dma((NZ,)),
            dma((NZ,)),
            dma((NZ,)),
            dma((NZ,)),
            dma((NTP,)),
            dma((NTP,)),
            dma((2,)),
            pltpu.SemaphoreType.REGULAR((3,)),
        ],
        compiler_params=pltpu.CompilerParams(collective_id=0, has_side_effects=True),
    )(*args)


def solution(mesh):
    return jax.shard_map(
        per_device,
        mesh=mesh,
        in_specs=(
            P(("gr", "sp"), "tp"),
            P(None, "tp"),
            P(None, "tp"),
            P(),
            P(),
            P(),
            P(None, "tp"),
            P(None, "tp"),
            P("gr", "tp", None),
            P("gr", "tp", None),
            P("gr"),
            P("tp", None),
        ),
        out_specs=(P("gr", None, "tp", "sp"), P("gr", "tp", None)),
        check_vma=False,
    )
```

```python
import functools
import jax
import jax.numpy as jnp
from jax import lax
from jax.experimental import pallas as pl
from jax.experimental.pallas import tpu as pltpu
from jax.sharding import PartitionSpec as P

H = 64
P_SIZE = 64
G = 16
N = 128
KW = 5
SPAN = 128
EPSILON = 1e-06
LEN = 8192
NY = 8
NZ = 4
NX = 4
NSP = 32
NTP = 8
TOK = 256
FEAT = 256
XC = 512
BC = 256
CC = 768
WC = 896
EDGE = 16
ROWS_A = 144
ROWS_B = TOK - ROWS_A
TOP = EDGE + ROWS_A
EARLY = 3

MESH = pl.DeviceIdType.MESH
F32 = jnp.float32
BF16 = jnp.bfloat16


def iota(shape, dim):
    return lax.broadcasted_iota(jnp.int32, shape, dim)


def kernel(
    inputs, x_weight, b_weight, dt_weight, dt_bias, decay_rate, conv_x, conv_b,
    query_c, query_gate, read_span, read_gain,
    cache, first_read,
    slab, wbuf, acc, proj, mixed, biasb, rateb, cxb, cbb, qb, gateb, gainb, rb,
    expand, sbuf, sendb, ybuf, redy, redz, reds, tot8,
    in_sem, load_sems, gsend, grecv, hsend, hrecv, asend, arecv,
    ysend, yrecv, zsend, zrecv, ssend, srecv, own_sem, stage,
):
    sp = lax.axis_index("sp")
    tp = lax.axis_index("tp")
    y = sp % NY
    z = sp // NY
    x = tp // 2
    core = tp % 2
    partner = 2 * x + 1 - core
    right = 2 * ((x + 1) % NX) + core
    left = 2 * ((x + NX - 1) % NX) + core
    across = 2 * ((x + 2) % NX) + core

    own_in = pltpu.make_async_copy(inputs, slab.at[tp, pl.ds(EDGE, TOK), :], in_sem)
    own_in.start()
    loads = [
        (x_weight, wbuf.at[:, pl.ds(0, XC)]),
        (b_weight, wbuf.at[:, pl.ds(XC, BC)]),
        (dt_weight, wbuf.at[:, pl.ds(CC, 128)]),
        (dt_bias, biasb),
        (decay_rate, rateb),
        (conv_x, cxb),
        (conv_b, cbb),
        (query_c, qb),
        (query_gate, gateb),
        (read_gain, gainb),
        (read_span, rb),
    ]
    copies = []
    for i, (src, dst) in enumerate(loads):
        c = pltpu.make_async_copy(src, dst, load_sems.at[i])
        c.start()
        copies.append(c)

    barrier = pltpu.get_barrier_semaphore()

    def at_y(other):
        return {"sp": z * NY + (other + NY) % NY}

    def greet_tp(i, carry):
        pl.semaphore_signal(
            barrier, inc=1, device_id={"tp": (tp + i) % NTP}, device_id_type=MESH
        )
        return carry

    def greet_z(i, carry):
        pl.semaphore_signal(
            barrier, inc=1, device_id={"sp": ((z + i) % NZ) * NY + y}, device_id_type=MESH
        )
        return carry

    lax.fori_loop(1, NTP, greet_tp, 0)
    lax.fori_loop(1, NZ, greet_z, 0)
    for side in (1, -1):
        pl.semaphore_signal(barrier, inc=1, device_id=at_y(y + side), device_id_type=MESH)
        pl.semaphore_signal(
            barrier, inc=1, device_id={"sp": (sp + NSP + side) % NSP}, device_id_type=MESH
        )

    def tell(index, distance):
        for side in (distance, -distance):
            pl.semaphore_signal(
                stage.at[index], inc=1, device_id=at_y(y + side), device_id_type=MESH
            )

    er = iota((256, 1024), 0) % 128
    ec = iota((256, 1024), 1)
    expand[...] = jnp.where(
        er == (ec // 512) * H + tp * 8 + (ec % 512) // P_SIZE, 1.0, 0.0
    ).astype(BF16)

    @pl.when(sp == 0)
    def _():
        slab[tp, pl.ds(0, EDGE), :] = jnp.zeros((EDGE, FEAT), BF16)

    own_in.wait()
    pl.semaphore_wait(barrier, NTP - 1 + NZ - 1 + 4)
    tell(0, 1)

    def edge_in():
        return pltpu.make_async_remote_copy(
            src_ref=slab.at[tp, pl.ds(TOK, EDGE), :],
            dst_ref=slab.at[tp, pl.ds(0, EDGE), :],
            send_sem=hsend.at[0],
            recv_sem=hrecv.at[0],
            device_id={"sp": (sp + 1) % NSP},
            device_id_type=MESH,
        )

    @pl.when(sp < NSP - 1)
    def _():
        edge_in().start()

    pieces = [(EDGE, ROWS_A), (0, EDGE), (TOP, ROWS_B)]
    sent = []

    def part(slot, j):
        return slab.at[slot, pl.ds(*pieces[j]), :]

    def forward(slot, j, dest, index):
        c = pltpu.make_async_remote_copy(
            src_ref=part(slot, j),
            dst_ref=part(slot, j),
            send_sem=gsend.at[index, j],
            recv_sem=grecv.at[slot, j],
            device_id={"tp": dest},
            device_id_type=MESH,
        )
        c.start()
        sent.append(c)

    def arrive(slot, j):
        pltpu.make_async_remote_copy(
            src_ref=part(slot, j),
            dst_ref=part(slot, j),
            send_sem=gsend.at[0, j],
            recv_sem=grecv.at[slot, j],
            device_id={"tp": partner},
            device_id_type=MESH,
        ).wait_recv()

    def send_own(j):
        for index, dest in enumerate((across, right, left, partner)):
            forward(tp, j, dest, index)

    ring = (right, left, across)

    def pass_on(j):
        for index, slot in enumerate(ring):
            arrive(slot, j)
            forward(slot, j, partner, 4 + index)

    def twin(slot):
        return slot + 1 - 2 * core

    def product(slot, start, count):
        rows = pl.ds(pl.multiple_of(slot * FEAT, FEAT), FEAT)
        return jnp.dot(
            slab[slot, pl.ds(start, count), :], wbuf[rows, :], preferred_element_type=F32
        )

    def add(slot, start, count):
        acc[pl.ds(start, count), :] += product(slot, start, count)

    send_own(0)
    for c in copies:
        c.wait()
    acc[pl.ds(TOP, ROWS_B), :] = product(tp, TOP, ROWS_B)

    @pl.when(sp > 0)
    def _():
        edge_in().wait_recv()

    send_own(1)
    send_own(2)
    acc[pl.ds(0, TOP), :] = product(tp, 0, TOP)
    for j in (0, 1):
        arrive(partner, j)
    add(partner, 0, TOP)
    pass_on(0)
    pl.semaphore_wait(stage.at[0], 2)
    tell(1, 2)
    pass_on(1)
    for slot in ring:
        add(slot, 0, TOP)
    for slot in ring[:2]:
        for j in (0, 1):
            arrive(twin(slot), j)
        add(twin(slot), 0, TOP)
    pl.semaphore_wait(stage.at[1], 2)
    tell(2, 1)
    for j in (0, 1):
        arrive(twin(across), j)
    last = product(twin(across), 0, TOP)
    proj[pl.ds(0, TOP), :] = (acc[pl.ds(0, TOP), :CC] + last[:, :CC]).astype(BF16).astype(F32)
    acc[pl.ds(0, TOP), CC:] += last[:, CC:]

    @pl.when(sp == 0)
    def _():
        proj[pl.ds(0, EDGE), :] = jnp.zeros((EDGE, CC), F32)

    def edge_down():
        return pltpu.make_async_remote_copy(
            src_ref=proj.at[pl.ds(EDGE, 8), :],
            dst_ref=proj.at[pl.ds(EDGE + TOK, 8), :],
            send_sem=hsend.at[1],
            recv_sem=hrecv.at[1],
            device_id={"sp": (sp + NSP - 1) % NSP},
            device_id_type=MESH,
        )

    @pl.when(sp > 0)
    def _():
        edge_down().start()

    bias = jnp.concatenate([biasb[0:1, :], biasb[1:2, :]], axis=1)
    rate = jnp.concatenate([rateb[0:1, :], rateb[1:2, :]], axis=1)
    row = iota((SPAN, SPAN), 0)
    col = iota((SPAN, SPAN), 1)
    later = jnp.where(col > row, 1.0, 0.0)
    earlier = jnp.where(col < row, 1.0, 0.0)

    def weights_of(k):
        dt_raw = acc[pl.ds(EDGE + k * SPAN, SPAN), CC:].astype(BF16).astype(F32)
        v = dt_raw + bias
        step = jnp.maximum(v, 0.0) + jnp.log1p(jnp.exp(-jnp.abs(v)))
        a = -(step * rate) / LEN
        tail = jnp.dot(later, a, precision=lax.Precision.HIGHEST, preferred_element_type=F32)
        head = jnp.dot(earlier, a, precision=lax.Precision.HIGHEST, preferred_element_type=F32)
        w = jnp.exp(jnp.where(col < H, tail, head)) * step
        redy[y, k : k + 1, pl.ds(512, 128)] = jnp.sum(a, axis=0, keepdims=True)
        high = w.astype(BF16)
        low = (w - high.astype(F32)).astype(BF16)
        return jnp.concatenate([high, low], axis=1)

    taps = [cxb[...].astype(F32), cbb[...].astype(F32)]

    def convolve(start, count):
        for block in range(CC // 256):
            tap = taps[0][:, block * 256 : (block + 1) * 256] if block < 2 else taps[1]
            cols = pl.ds(block * 256, 256)
            total = jnp.zeros((count, 256), F32)
            for o in range(KW):
                total = total + tap[o : o + 1] * proj[pl.ds(start + EDGE - 2 + o, count), cols]
            mixed[pl.ds(start, count), cols] = jax.nn.silu(total).astype(BF16)

    order = (4 * (row % 32) + row // 32 == col)
    order_t = jnp.where(order, 1.0, 0.0).astype(BF16)
    contract_last = (((1,), (1,)), ((), ()))
    queries = []
    for g in range(2):
        q8 = jnp.broadcast_to(qb[0, g : g + 1, :].astype(F32), (8, N)).astype(BF16)
        queries.append(
            lax.dot_general(q8, order_t, contract_last, preferred_element_type=F32).astype(BF16)
        )
    half = iota((32, 128), 1) < P_SIZE
    chosen = rb[0]

    def state_copy(k, d, s):
        return pltpu.make_async_remote_copy(
            src_ref=sendb.at[d, k],
            dst_ref=cache.at[2 * s + k],
            send_sem=asend.at[k, d],
            recv_sem=arecv.at[k, s],
            device_id={"sp": d},
            device_id_type=MESH,
        )

    def send_states(k, first, last):
        def body(i, carry):
            m = 7 - (first + i // NZ)
            dy = (m % 2) * ((m + 1) // 2) + (1 - m % 2) * (8 - m // 2)
            d = ((z + i % NZ) % NZ) * NY + (y + dy) % NY
            state_copy(k, d, sp).start()
            return carry

        lax.fori_loop(0, (last - first) * NZ, body, 0)

    def send_column(k):
        def body(i, carry):
            state_copy(k, ((z + i) % NZ) * NY + y, sp).start()
            return carry

        lax.fori_loop(1, NZ, body, 0)

    own_out = []

    def states_of(k, pair):
        rows = pl.ds(k * SPAN, SPAN)
        keys_t = [
            lax.dot_general(
                order_t, mixed[rows, pl.ds(XC + g * N, N)], contract_last,
                preferred_element_type=F32,
            ).astype(BF16)
            for g in range(2)
        ]
        for e in range(2):
            wide = jnp.dot(pair, expand[:, pl.ds(e * 512, 512)], preferred_element_type=F32)
            weighted = (mixed[rows, pl.ds(0, XC)].astype(F32) * wide).astype(BF16)
            for g in range(2):
                state = jnp.dot(
                    keys_t[g], weighted[:, g * 256 : (g + 1) * 256], preferred_element_type=F32
                )
                read = jnp.dot(queries[g], state.astype(BF16), preferred_element_type=F32)
                ybuf[e : e + 1, pl.ds(g * 256, 256)] = read[0:1]
                for j in range(2):
                    for a in range(2):
                        one = state[64 * a : 64 * a + 32, 128 * j : 128 * j + 128]
                        two = state[64 * a + 32 : 64 * a + 64, 128 * j : 128 * j + 128]
                        first = jnp.where(half, one, pltpu.roll(two, 64, 1))
                        second = jnp.where(half, pltpu.roll(one, 64, 1), two)
                        h = 4 * g + 2 * j
                        sbuf[a, pl.ds(h, 32, stride=8), :] = first
                        sbuf[a, pl.ds(h + 1, 32, stride=8), :] = second
            for a in range(2):
                sendb[:, k, e, :, pl.ds(a * 128, 128)] = (
                    sbuf[a].reshape(NSP, 8, 128).astype(BF16)
                )
        at = jnp.full((1, 512), 2 * sp + k, jnp.int32)
        pick = jnp.full((1, 512), chosen, jnp.int32)
        redy[y, k : k + 1, pl.ds(0, 512)] = jnp.where(at <= pick, ybuf[0:1, :], 0.0) + jnp.where(
            at >= pick, ybuf[1:2, :], 0.0
        )
        c = pltpu.make_async_copy(sendb.at[sp, k], cache.at[2 * sp + k], own_sem.at[k])
        c.start()
        own_out.append(c)

    pair = weights_of(0)
    for first in range(0, SPAN, 16):
        convolve(first, 16)
    pass_on(2)
    pl.semaphore_wait(stage.at[2], 2)
    states_of(0, pair)
    send_column(0)
    send_states(0, 0, EARLY)

    for slot in (partner, *ring, twin(right), twin(left)):
        if slot is not right and slot is not left and slot is not across:
            arrive(slot, 2)
        add(slot, TOP, ROWS_B)
    arrive(twin(across), 2)
    last = product(twin(across), TOP, ROWS_B)
    rest = pl.ds(TOP, ROWS_B)
    proj[rest, :] = (acc[rest, :CC] + last[:, :CC]).astype(BF16).astype(F32)
    acc[rest, CC:] += last[:, CC:]
    pair = weights_of(1)
    for first in range(SPAN, TOK - 16, 16):
        convolve(first, 16)

    @pl.when(sp < NSP - 1)
    def _():
        edge_down().wait_recv()

    @pl.when(sp == NSP - 1)
    def _():
        proj[pl.ds(EDGE + TOK, 8), :] = jnp.zeros((8, CC), F32)

    convolve(TOK - 16, 16)
    states_of(1, pair)

    def y_copy(d, s):
        return pltpu.make_async_remote_copy(
            src_ref=redy.at[s],
            dst_ref=redy.at[s],
            send_sem=ysend.at[d],
            recv_sem=yrecv.at[s],
            device_id=at_y(d),
            device_id_type=MESH,
        )

    def z_copy(d, s):
        return pltpu.make_async_remote_copy(
            src_ref=redz.at[s],
            dst_ref=redz.at[s],
            send_sem=zsend.at[d],
            recv_sem=zrecv.at[s],
            device_id={"sp": d * NY + y},
            device_id_type=MESH,
        )

    def s_copy(d, s):
        return pltpu.make_async_remote_copy(
            src_ref=reds.at[s],
            dst_ref=reds.at[s],
            send_sem=ssend.at[d],
            recv_sem=srecv.at[s],
            device_id={"tp": d},
            device_id_type=MESH,
        )

    def each(copy, me, count, act):
        def body(i, carry):
            act(copy, me, (me + i) % count)
            return carry

        lax.fori_loop(1, count, body, 0)

    def start(copy, me, other):
        copy(other, me).start()

    def receive(copy, me, other):
        copy(other, other).wait_recv()

    def leave(copy, me, other):
        copy(other, me).wait_send()

    each(y_copy, y, NY, start)
    send_states(0, EARLY, 7)
    send_column(1)
    send_states(1, 0, 7)

    def spread(rows):
        high = rows.astype(BF16)
        low = (rows - high.astype(F32)).astype(BF16)
        return jnp.dot(
            jnp.concatenate([high, low], axis=1),
            expand[:, pl.ds(0, 512)],
            preferred_element_type=F32,
        )

    gate = jax.nn.silu(gateb[0].astype(F32))
    each(y_copy, y, NY, receive)
    base = 2 * NY * z
    ahead_lane = iota((8, 128), 1) < H
    block_log = jnp.zeros((8, 128), F32)
    span_logs = [jnp.zeros((8, 128), F32), jnp.zeros((8, 128), F32)]
    pick = jnp.full((8, 128), chosen, jnp.int32)
    span_at = [base + 2 * iota((8, 128), 0) + k for k in range(2)]
    for other in range(2 * NY):
        log = jnp.broadcast_to(
            redy[other // 2, other % 2 : other % 2 + 1, pl.ds(512, 128)], (8, 128)
        )
        here = jnp.full((8, 128), base + other, jnp.int32)
        log = jnp.where(ahead_lane, jnp.where(here <= pick, log, 0.0), jnp.where(here >= pick, log, 0.0))
        block_log = block_log + log
        for k in range(2):
            counted = jnp.where(
                ahead_lane,
                jnp.where(here > span_at[k], log, 0.0),
                jnp.where(here < span_at[k], log, 0.0),
            )
            span_logs[k] = span_logs[k] + counted
    span_weights = [jnp.exp(t + pltpu.roll(t, H, 1)) for t in span_logs]
    wide_weight = spread(jnp.concatenate(span_weights, axis=0))
    partial = jnp.zeros((8, 512), F32)
    for k in range(2):
        partial = partial + wide_weight[8 * k : 8 * k + 8] * redy[:, k, pl.ds(0, 512)]
    redz[z, :, pl.ds(0, 512)] = jnp.sum(partial, axis=0, keepdims=True)
    redz[z, :, pl.ds(512, 128)] = block_log[0:1]
    each(z_copy, z, NZ, start)
    each(z_copy, z, NZ, receive)
    lane = iota((1, 128), 1)
    block_rows = []
    for block in range(NZ):
        after = jnp.zeros((1, 128), F32)
        before = jnp.zeros((1, 128), F32)
        for other in range(block + 1, NZ):
            after = after + redz[other, :, pl.ds(512, 128)]
        for other in range(block):
            before = before + redz[other, :, pl.ds(512, 128)]
        block_rows.append(jnp.where(lane < H, after, before))
    block_rows = block_rows + [jnp.zeros((8 - NZ, 128), F32)]
    logs = jnp.concatenate(block_rows, axis=0)
    block_factor = spread(jnp.exp(logs + pltpu.roll(logs, H, 1)))
    total = jnp.zeros((1, 512), F32)
    for block in range(NZ):
        total = total + block_factor[block : block + 1] * redz[block, :, pl.ds(0, 512)]
    for h in range(8):
        tot8[h : h + 1, :] = total[:, h * P_SIZE : (h + 1) * P_SIZE]
    gated = tot8[...] * gate
    squares = jnp.sum(jnp.sum(gated * gated, axis=0, keepdims=True), axis=1, keepdims=True)
    reds[tp] = jnp.broadcast_to(squares, (1, 128))
    each(s_copy, tp, NTP, start)
    each(s_copy, tp, NTP, receive)
    square_sum = jnp.sum(reds[...], axis=0)[:, :64]
    scale = lax.rsqrt(square_sum / (H * P_SIZE) + EPSILON)
    first_read[0] = (gated * scale * gainb[...]).astype(BF16)

    for c in sent:
        c.wait_send()

    @pl.when(sp < NSP - 1)
    def _():
        edge_in().wait_send()

    @pl.when(sp > 0)
    def _():
        edge_down().wait_send()

    each(y_copy, y, NY, leave)
    each(z_copy, z, NZ, leave)
    each(s_copy, tp, NTP, leave)
    for k in range(2):
        each(functools.partial(state_copy, k), sp, NSP, receive)
        each(functools.partial(state_copy, k), sp, NSP, leave)
        own_out[k].wait()


def per_device(*args):
    dma = pltpu.SemaphoreType.DMA
    any_spec = pl.BlockSpec(memory_space=pl.ANY)
    vmem_spec = pl.BlockSpec(memory_space=pltpu.VMEM)
    shapes = (
        jax.ShapeDtypeStruct((64, 2, 8, 256), BF16),
        jax.ShapeDtypeStruct((1, 8, 64), BF16),
    )
    return pl.pallas_call(
        kernel,
        out_shape=tuple(pltpu.VMEM(t.shape, t.dtype) for t in shapes),
        in_specs=[any_spec] * 12,
        out_specs=(vmem_spec, vmem_spec),
        scratch_shapes=[
            pltpu.VMEM((NTP, EDGE + TOK, FEAT), BF16),
            pltpu.VMEM((2048, WC), BF16),
            pltpu.VMEM((EDGE + TOK, WC), F32),
            pltpu.VMEM((EDGE + TOK + 8, CC), F32),
            pltpu.VMEM((TOK, CC), BF16),
            pltpu.VMEM((2, H), F32),
            pltpu.VMEM((2, H), F32),
            pltpu.VMEM((KW, XC), BF16),
            pltpu.VMEM((KW, BC), BF16),
            pltpu.VMEM((1, 2, N), BF16),
            pltpu.VMEM((1, 8, P_SIZE), BF16),
            pltpu.VMEM((8, P_SIZE), F32),
            pltpu.SMEM((1,), jnp.int32),
            pltpu.VMEM((256, 1024), BF16),
            pltpu.VMEM((2, 256, 128), F32),
            pltpu.VMEM((NSP, 2, 2, 8, 256), BF16),
            pltpu.VMEM((8, 512), F32),
            pltpu.VMEM((NY, 2, 640), F32),
            pltpu.VMEM((NZ, 1, 640), F32),
            pltpu.VMEM((NTP, 1, 128), F32),
            pltpu.VMEM((8, P_SIZE), F32),
            dma,
            dma((11,)),
            dma((7, 3)),
            dma((NTP, 3)),
            dma((2,)),
            dma((2,)),
            dma((2, NSP)),
            dma((2, NSP)),
            dma((NY,)),
            dma((NY,)),
            dma((NZ,)),
            dma((NZ,)),
            dma((NTP,)),
            dma((NTP,)),
            dma((2,)),
            pltpu.SemaphoreType.REGULAR((3,)),
        ],
        compiler_params=pltpu.CompilerParams(collective_id=0, has_side_effects=True),
    )(*args)


def solution(mesh):
    return jax.shard_map(
        per_device,
        mesh=mesh,
        in_specs=(
            P(("gr", "sp"), "tp"),
            P(None, "tp"),
            P(None, "tp"),
            P(),
            P(),
            P(),
            P(None, "tp"),
            P(None, "tp"),
            P("gr", "tp", None),
            P("gr", "tp", None),
            P("gr"),
            P("tp", None),
        ),
        out_specs=(P("gr", None, "tp", "sp"), P("gr", "tp", None)),
        check_vma=False,
    )
```

```python
import jax
import jax.numpy as jnp
from jax import lax
from jax.experimental import pallas as pl
from jax.experimental.pallas import tpu as pltpu
from jax.sharding import PartitionSpec as P

H = 64
P_SIZE = 64
G = 16
N = 128
KW = 5
SPAN = 128
EPSILON = 1e-06
LEN = 8192
NY = 8
NZ = 4
NX = 4
NSP = 32
NTP = 8
TOK = 256
FEAT = 256
XC = 512
BC = 256
CC = 768
WC = 896
EDGE = 16
ROWS_A = 144
ROWS_B = TOK - ROWS_A
TOP = EDGE + ROWS_A
EARLY = 3
MID = 0

MESH = pl.DeviceIdType.MESH
F32 = jnp.float32
BF16 = jnp.bfloat16


def iota(shape, dim):
    return lax.broadcasted_iota(jnp.int32, shape, dim)


def kernel(
    inputs, x_weight, b_weight, dt_weight, dt_bias, decay_rate, conv_x, conv_b,
    query_c, query_gate, read_span, read_gain,
    cache, first_read,
    slab, wbuf, acc, proj, mixed, held, biasb, rateb, cxb, cbb, qb, gateb, gainb, rb,
    expand, sbuf, sendb, ybuf, redy, redz, reds, tot8,
    in_sem, load_sems, gsend, grecv, hsend, hrecv, asend, arecv,
    ysems, zsems, ssems, own_sem, stage,
):
    sp = lax.axis_index("sp")
    tp = lax.axis_index("tp")
    y = sp % NY
    z = sp // NY
    x = tp // 2
    core = tp % 2
    partner = 2 * x + 1 - core
    right = 2 * ((x + 1) % NX) + core
    left = 2 * ((x + NX - 1) % NX) + core
    across = 2 * ((x + 2) % NX) + core

    own_in = pltpu.make_async_copy(inputs, slab.at[tp, pl.ds(EDGE, TOK), :], in_sem)
    own_in.start()
    loads = [
        (x_weight, wbuf.at[:, pl.ds(0, XC)]),
        (b_weight, wbuf.at[:, pl.ds(XC, BC)]),
        (dt_weight, wbuf.at[:, pl.ds(CC, 128)]),
        (dt_bias, biasb),
        (decay_rate, rateb),
        (conv_x, cxb),
        (conv_b, cbb),
        (query_c, qb),
        (query_gate, gateb),
        (read_gain, gainb),
        (read_span, rb),
    ]
    copies = []
    for i, (src, dst) in enumerate(loads):
        c = pltpu.make_async_copy(src, dst, load_sems.at[i])
        c.start()
        copies.append(c)

    barrier = pltpu.get_barrier_semaphore()

    def at_y(other):
        return {"sp": z * NY + (other + NY) % NY}

    def greet_tp(i, carry):
        pl.semaphore_signal(
            barrier, inc=1, device_id={"tp": (tp + i) % NTP}, device_id_type=MESH
        )
        return carry

    def greet_z(i, carry):
        pl.semaphore_signal(
            barrier, inc=1, device_id={"sp": ((z + i) % NZ) * NY + y}, device_id_type=MESH
        )
        return carry

    lax.fori_loop(1, NTP, greet_tp, 0)
    lax.fori_loop(1, NZ, greet_z, 0)
    for side in (1, -1):
        pl.semaphore_signal(barrier, inc=1, device_id=at_y(y + side), device_id_type=MESH)
        pl.semaphore_signal(
            barrier, inc=1, device_id={"sp": (sp + NSP + side) % NSP}, device_id_type=MESH
        )

    def tell(index, distance):
        for side in (distance, -distance):
            pl.semaphore_signal(
                stage.at[index], inc=1, device_id=at_y(y + side), device_id_type=MESH
            )

    @pl.when(sp == 0)
    def _():
        slab[tp, pl.ds(0, EDGE), :] = jnp.zeros((EDGE, FEAT), BF16)

    own_in.wait()
    pl.semaphore_wait(barrier, NTP - 1 + NZ - 1 + 4)
    tell(0, 1)

    def edge_in():
        return pltpu.make_async_remote_copy(
            src_ref=slab.at[tp, pl.ds(TOK, EDGE), :],
            dst_ref=slab.at[tp, pl.ds(0, EDGE), :],
            send_sem=hsend.at[0],
            recv_sem=hrecv.at[0],
            device_id={"sp": (sp + 1) % NSP},
            device_id_type=MESH,
        )

    @pl.when(sp < NSP - 1)
    def _():
        edge_in().start()

    pieces = [(EDGE, ROWS_A), (0, EDGE), (TOP, ROWS_B)]

    def part(slot, j):
        return slab.at[slot, pl.ds(*pieces[j]), :]

    def forward(slot, j, dest):
        c = pltpu.make_async_remote_copy(
            src_ref=part(slot, j),
            dst_ref=part(slot, j),
            send_sem=gsend.at[j],
            recv_sem=grecv.at[slot, j],
            device_id={"tp": dest},
            device_id_type=MESH,
        )
        c.start()

    def arrive(slot, j):
        pltpu.make_async_remote_copy(
            src_ref=part(slot, j),
            dst_ref=part(slot, j),
            send_sem=gsend.at[j],
            recv_sem=grecv.at[slot, j],
            device_id={"tp": partner},
            device_id_type=MESH,
        ).wait_recv()

    def send_own(j):
        for dest in (across, right, left, partner):
            forward(tp, j, dest)

    ring = (right, left, across)

    def pass_on(j):
        for slot in ring:
            arrive(slot, j)
            forward(slot, j, partner)

    def twin(slot):
        return slot + 1 - 2 * core

    def product(slot, start, count):
        rows = pl.ds(pl.multiple_of(slot * FEAT, FEAT), FEAT)
        return jnp.dot(
            slab[slot, pl.ds(start, count), :], wbuf[rows, :], preferred_element_type=F32
        )

    def add(slot, start, count):
        acc[pl.ds(start, count), :] += product(slot, start, count)

    send_own(0)
    er = iota((256, 1024), 0) % 128
    ec = iota((256, 1024), 1)
    expand[...] = jnp.where(
        er == (ec // 512) * H + tp * 8 + (ec % 512) // P_SIZE, 1.0, 0.0
    ).astype(BF16)

    @pl.when(sp > 0)
    def _():
        edge_in().wait_recv()

    send_own(1)
    send_own(2)
    for c in copies:
        c.wait()
    acc[pl.ds(TOP, ROWS_B), :] = product(tp, TOP, ROWS_B)
    acc[pl.ds(0, TOP), :] = product(tp, 0, TOP)
    for j in (0, 1):
        arrive(partner, j)
    add(partner, 0, TOP)
    pass_on(0)
    pl.semaphore_wait(stage.at[0], 2)
    tell(1, 2)
    pass_on(1)
    for slot in ring:
        add(slot, 0, TOP)
    for slot in ring[:2]:
        for j in (0, 1):
            arrive(twin(slot), j)
        add(twin(slot), 0, TOP)
    pl.semaphore_wait(stage.at[1], 2)
    tell(2, 1)
    for j in (0, 1):
        arrive(twin(across), j)
    last = product(twin(across), 0, TOP)
    proj[pl.ds(0, TOP), :] = (acc[pl.ds(0, TOP), :CC] + last[:, :CC]).astype(BF16).astype(F32)
    acc[pl.ds(0, TOP), CC:] += last[:, CC:]

    @pl.when(sp == 0)
    def _():
        proj[pl.ds(0, EDGE), :] = jnp.zeros((EDGE, CC), F32)

    def edge_down():
        return pltpu.make_async_remote_copy(
            src_ref=proj.at[pl.ds(EDGE, 8), :],
            dst_ref=proj.at[pl.ds(EDGE + TOK, 8), :],
            send_sem=hsend.at[1],
            recv_sem=hrecv.at[1],
            device_id={"sp": (sp + NSP - 1) % NSP},
            device_id_type=MESH,
        )

    @pl.when(sp > 0)
    def _():
        edge_down().start()

    bias = jnp.concatenate([biasb[0:1, :], biasb[1:2, :]], axis=1)
    rate = jnp.concatenate([rateb[0:1, :], rateb[1:2, :]], axis=1)
    row = iota((SPAN, SPAN), 0)
    col = iota((SPAN, SPAN), 1)
    later = jnp.where(col > row, 1.0, 0.0)
    earlier = jnp.where(col < row, 1.0, 0.0)

    def weights_of(k):
        dt_raw = acc[pl.ds(EDGE + k * SPAN, SPAN), CC:].astype(BF16).astype(F32)
        v = dt_raw + bias
        step = jnp.maximum(v, 0.0) + jnp.log1p(jnp.exp(-jnp.abs(v)))
        a = -(step * rate) / LEN
        tail = jnp.dot(later, a, precision=lax.Precision.HIGHEST, preferred_element_type=F32)
        head = jnp.dot(earlier, a, precision=lax.Precision.HIGHEST, preferred_element_type=F32)
        w = jnp.exp(jnp.where(col < H, tail, head)) * step
        redy[y, k : k + 1, pl.ds(512, 128)] = jnp.sum(a, axis=0, keepdims=True)
        high = w.astype(BF16)
        low = (w - high.astype(F32)).astype(BF16)
        return jnp.concatenate([high, low], axis=1)

    taps = [cxb[...].astype(F32), cbb[...].astype(F32)]

    def convolve(start, count):
        for block in range(CC // 256):
            tap = taps[0][:, block * 256 : (block + 1) * 256] if block < 2 else taps[1]
            cols = pl.ds(block * 256, 256)
            total = jnp.zeros((count, 256), F32)
            for o in range(KW):
                total = total + tap[o : o + 1] * proj[pl.ds(start + EDGE - 2 + o, count), cols]
            mixed[pl.ds(start, count), cols] = jax.nn.silu(total).astype(BF16)

    order = (4 * (row % 32) + row // 32 == col)
    order_t = jnp.where(order, 1.0, 0.0).astype(BF16)
    contract_last = (((1,), (1,)), ((), ()))
    queries = []
    for g in range(2):
        q8 = jnp.broadcast_to(qb[0, g : g + 1, :].astype(F32), (8, N)).astype(BF16)
        queries.append(
            lax.dot_general(q8, order_t, contract_last, preferred_element_type=F32).astype(BF16)
        )
    half = iota((32, 128), 1) < P_SIZE
    chosen = rb[0]

    def state_copy(k, d, s):
        return pltpu.make_async_remote_copy(
            src_ref=sendb.at[d, k],
            dst_ref=cache.at[2 * s + k],
            send_sem=asend,
            recv_sem=arecv,
            device_id={"sp": d},
            device_id_type=MESH,
        )

    across_y = [lax.rem(y + dy, NY) for dy in range(NY)]
    across_z = [lax.rem(z + dz, NZ) * NY for dz in range(NZ)]
    distances = (4, 5, 3, 6, 2, 7, 1)

    def send_states(k, first, last):
        for dy in distances[first:last]:
            for dz in range(NZ):
                state_copy(k, across_z[dz] + across_y[dy], sp).start()

    def send_column(k):
        for dz in range(1, NZ):
            state_copy(k, across_z[dz] + y, sp).start()

    own_out = []

    def states_of(k, pair):
        rows = pl.ds(k * SPAN, SPAN)
        keys_t = [
            lax.dot_general(
                order_t, mixed[rows, pl.ds(XC + g * N, N)], contract_last,
                preferred_element_type=F32,
            ).astype(BF16)
            for g in range(2)
        ]
        for e in range(2):
            wide = jnp.dot(pair, expand[:, pl.ds(e * 512, 512)], preferred_element_type=F32)
            weighted = (mixed[rows, pl.ds(0, XC)].astype(F32) * wide).astype(BF16)
            for g in range(2):
                state = jnp.dot(
                    keys_t[g], weighted[:, g * 256 : (g + 1) * 256], preferred_element_type=F32
                )
                read = jnp.dot(queries[g], state.astype(BF16), preferred_element_type=F32)
                ybuf[e : e + 1, pl.ds(g * 256, 256)] = read[0:1]
                held[e, g] = state
        at = jnp.full((1, 512), 2 * sp + k, jnp.int32)
        pick = jnp.full((1, 512), chosen, jnp.int32)
        redy[y, k : k + 1, pl.ds(0, 512)] = jnp.where(at <= pick, ybuf[0:1, :], 0.0) + jnp.where(
            at >= pick, ybuf[1:2, :], 0.0
        )

    def arrange(k):
        for e in range(2):
            for g in range(2):
                for j in range(2):
                    for a in range(2):
                        lanes = pl.ds(128 * j, 128)
                        one = held[e, g, pl.ds(64 * a, 32), lanes]
                        two = held[e, g, pl.ds(64 * a + 32, 32), lanes]
                        first = jnp.where(half, one, pltpu.roll(two, 64, 1))
                        second = jnp.where(half, pltpu.roll(one, 64, 1), two)
                        h = 4 * g + 2 * j
                        sbuf[a, pl.ds(h, 32, stride=8), :] = first
                        sbuf[a, pl.ds(h + 1, 32, stride=8), :] = second
            for a in range(2):
                sendb[:, k, e, :, pl.ds(a * 128, 128)] = (
                    sbuf[a].reshape(NSP, 8, 128).astype(BF16)
                )
        c = pltpu.make_async_copy(sendb.at[sp, k], cache.at[2 * sp + k], own_sem.at[k])
        c.start()
        own_out.append(c)

    pair = weights_of(0)
    for first in range(0, SPAN, 16):
        convolve(first, 16)
    pass_on(2)
    pl.semaphore_wait(stage.at[2], 2)
    states_of(0, pair)
    arrange(0)
    send_column(0)
    send_states(0, 0, EARLY)

    for slot in (partner, *ring, twin(right), twin(left)):
        if slot is not right and slot is not left and slot is not across:
            arrive(slot, 2)
        add(slot, TOP, ROWS_B)
    arrive(twin(across), 2)
    last = product(twin(across), TOP, ROWS_B)
    rest = pl.ds(TOP, ROWS_B)
    proj[rest, :] = (acc[rest, :CC] + last[:, :CC]).astype(BF16).astype(F32)
    acc[rest, CC:] += last[:, CC:]
    pair = weights_of(1)
    for first in range(SPAN, TOK - 16, 16):
        convolve(first, 16)

    @pl.when(sp < NSP - 1)
    def _():
        edge_down().wait_recv()

    @pl.when(sp == NSP - 1)
    def _():
        proj[pl.ds(EDGE + TOK, 8), :] = jnp.zeros((8, CC), F32)

    convolve(TOK - 16, 16)
    states_of(1, pair)

    def exchange(buffer, me, count, sems, place):
        for i in range(1, count):
            other = lax.rem(me + i, count)
            pltpu.make_async_remote_copy(
                src_ref=buffer.at[me],
                dst_ref=buffer.at[me],
                send_sem=sems.at[0],
                recv_sem=sems.at[1],
                device_id=place(other),
                device_id_type=MESH,
            ).start()

        return pltpu.make_async_remote_copy(
            src_ref=buffer.at[pl.ds(0, count - 1)],
            dst_ref=buffer.at[pl.ds(0, count - 1)],
            send_sem=sems.at[0],
            recv_sem=sems.at[1],
            device_id=place(me),
            device_id_type=MESH,
        )

    y_all = exchange(redy, y, NY, ysems, lambda d: {"sp": z * NY + d})
    send_states(0, EARLY, 7)
    arrange(1)
    send_column(1)
    send_states(1, 0, MID)

    def spread(rows):
        high = rows.astype(BF16)
        low = (rows - high.astype(F32)).astype(BF16)
        return jnp.dot(
            jnp.concatenate([high, low], axis=1),
            expand[:, pl.ds(0, 512)],
            preferred_element_type=F32,
        )

    gate = jax.nn.silu(gateb[0].astype(F32))
    y_all.wait_recv()
    base = 2 * NY * z
    ahead_lane = iota((8, 128), 1) < H
    block_log = jnp.zeros((8, 128), F32)
    span_logs = [jnp.zeros((8, 128), F32), jnp.zeros((8, 128), F32)]
    pick = jnp.full((8, 128), chosen, jnp.int32)
    span_at = [base + 2 * iota((8, 128), 0) + k for k in range(2)]
    for other in range(2 * NY):
        log = jnp.broadcast_to(
            redy[other // 2, other % 2 : other % 2 + 1, pl.ds(512, 128)], (8, 128)
        )
        here = jnp.full((8, 128), base + other, jnp.int32)
        log = jnp.where(ahead_lane, jnp.where(here <= pick, log, 0.0), jnp.where(here >= pick, log, 0.0))
        block_log = block_log + log
        for k in range(2):
            counted = jnp.where(
                ahead_lane,
                jnp.where(here > span_at[k], log, 0.0),
                jnp.where(here < span_at[k], log, 0.0),
            )
            span_logs[k] = span_logs[k] + counted
    span_weights = [jnp.exp(t + pltpu.roll(t, H, 1)) for t in span_logs]
    wide_weight = spread(jnp.concatenate(span_weights, axis=0))
    partial = jnp.zeros((8, 512), F32)
    for k in range(2):
        partial = partial + wide_weight[8 * k : 8 * k + 8] * redy[:, k, pl.ds(0, 512)]
    redz[z, :, pl.ds(0, 512)] = jnp.sum(partial, axis=0, keepdims=True)
    redz[z, :, pl.ds(512, 128)] = block_log[0:1]
    z_all = exchange(redz, z, NZ, zsems, lambda d: {"sp": d * NY + y})
    send_states(1, MID, 7)
    z_all.wait_recv()
    lane = iota((1, 128), 1)
    block_rows = []
    for block in range(NZ):
        after = jnp.zeros((1, 128), F32)
        before = jnp.zeros((1, 128), F32)
        for other in range(block + 1, NZ):
            after = after + redz[other, :, pl.ds(512, 128)]
        for other in range(block):
            before = before + redz[other, :, pl.ds(512, 128)]
        block_rows.append(jnp.where(lane < H, after, before))
    block_rows = block_rows + [jnp.zeros((8 - NZ, 128), F32)]
    logs = jnp.concatenate(block_rows, axis=0)
    block_factor = spread(jnp.exp(logs + pltpu.roll(logs, H, 1)))
    total = jnp.zeros((1, 512), F32)
    for block in range(NZ):
        total = total + block_factor[block : block + 1] * redz[block, :, pl.ds(0, 512)]
    for h in range(8):
        tot8[h : h + 1, :] = total[:, h * P_SIZE : (h + 1) * P_SIZE]
    gated = tot8[...] * gate
    squares = jnp.sum(jnp.sum(gated * gated, axis=0, keepdims=True), axis=1, keepdims=True)
    reds[tp] = jnp.broadcast_to(squares, (1, 128))
    s_all = exchange(reds, tp, NTP, ssems, lambda d: {"tp": d})
    s_all.wait_recv()
    square_sum = jnp.sum(reds[...], axis=0)[:, :64]
    scale = lax.rsqrt(square_sum / (H * P_SIZE) + EPSILON)
    first_read[0] = (gated * scale * gainb[...]).astype(BF16)

    for j, (start, count) in enumerate(pieces):
        sent = slab.at[pl.ds(0, NTP - 1), pl.ds(start, count), :]
        pltpu.make_async_remote_copy(
            src_ref=sent,
            dst_ref=sent,
            send_sem=gsend.at[j],
            recv_sem=gsend.at[j],
            device_id={"tp": partner},
            device_id_type=MESH,
        ).wait_send()

    @pl.when(sp < NSP - 1)
    def _():
        edge_in().wait_send()

    @pl.when(sp > 0)
    def _():
        edge_down().wait_send()

    y_all.wait_send()
    z_all.wait_send()
    s_all.wait_send()
    every = cache.at[pl.ds(0, 2 * NSP - 2)]
    states = pltpu.make_async_remote_copy(
        src_ref=every,
        dst_ref=every,
        send_sem=asend,
        recv_sem=arecv,
        device_id={"sp": sp},
        device_id_type=MESH,
    )
    states.wait_recv()
    states.wait_send()
    for c in own_out:
        c.wait()


def per_device(*args):
    dma = pltpu.SemaphoreType.DMA
    any_spec = pl.BlockSpec(memory_space=pl.ANY)
    vmem_spec = pl.BlockSpec(memory_space=pltpu.VMEM)
    shapes = (
        jax.ShapeDtypeStruct((64, 2, 8, 256), BF16),
        jax.ShapeDtypeStruct((1, 8, 64), BF16),
    )
    return pl.pallas_call(
        kernel,
        out_shape=tuple(pltpu.VMEM(t.shape, t.dtype) for t in shapes),
        in_specs=[any_spec] * 12,
        out_specs=(vmem_spec, vmem_spec),
        scratch_shapes=[
            pltpu.VMEM((NTP, EDGE + TOK, FEAT), BF16),
            pltpu.VMEM((2048, WC), BF16),
            pltpu.VMEM((EDGE + TOK, WC), F32),
            pltpu.VMEM((EDGE + TOK + 8, CC), F32),
            pltpu.VMEM((TOK, CC), BF16),
            pltpu.VMEM((2, 2, N, 256), F32),
            pltpu.VMEM((2, H), F32),
            pltpu.VMEM((2, H), F32),
            pltpu.VMEM((KW, XC), BF16),
            pltpu.VMEM((KW, BC), BF16),
            pltpu.VMEM((1, 2, N), BF16),
            pltpu.VMEM((1, 8, P_SIZE), BF16),
            pltpu.VMEM((8, P_SIZE), F32),
            pltpu.SMEM((1,), jnp.int32),
            pltpu.VMEM((256, 1024), BF16),
            pltpu.VMEM((2, 256, 128), F32),
            pltpu.VMEM((NSP, 2, 2, 8, 256), BF16),
            pltpu.VMEM((8, 512), F32),
            pltpu.VMEM((NY, 2, 640), F32),
            pltpu.VMEM((NZ, 1, 640), F32),
            pltpu.VMEM((NTP, 1, 128), F32),
            pltpu.VMEM((8, P_SIZE), F32),
            dma,
            dma((11,)),
            dma((3,)),
            dma((NTP, 3)),
            dma((2,)),
            dma((2,)),
            dma,
            dma,
            dma((2,)),
            dma((2,)),
            dma((2,)),
            dma((2,)),
            pltpu.SemaphoreType.REGULAR((3,)),
        ],
        compiler_params=pltpu.CompilerParams(collective_id=0, has_side_effects=True),
    )(*args)


def solution(mesh):
    return jax.shard_map(
        per_device,
        mesh=mesh,
        in_specs=(
            P(("gr", "sp"), "tp"),
            P(None, "tp"),
            P(None, "tp"),
            P(),
            P(),
            P(),
            P(None, "tp"),
            P(None, "tp"),
            P("gr", "tp", None),
            P("gr", "tp", None),
            P("gr"),
            P("tp", None),
        ),
        out_specs=(P("gr", None, "tp", "sp"), P("gr", "tp", None)),
        check_vma=False,
    )
```

```python
import jax
import jax.numpy as jnp
from jax import lax
from jax.experimental import pallas as pl
from jax.experimental.pallas import tpu as pltpu
from jax.sharding import PartitionSpec as P

H = 64
P_SIZE = 64
G = 16
N = 128
KW = 5
SPAN = 128
EPSILON = 1e-06
LEN = 8192
NY = 8
NZ = 4
NX = 4
NSP = 32
NTP = 8
TOK = 256
FEAT = 256
XC = 512
BC = 256
CC = 768
WC = 896
EDGE = 16
ROWS_A = 144
ROWS_B = TOK - ROWS_A
TOP = EDGE + ROWS_A
EARLY = 2
MID = 0

MESH = pl.DeviceIdType.MESH
F32 = jnp.float32
BF16 = jnp.bfloat16


def iota(shape, dim):
    return lax.broadcasted_iota(jnp.int32, shape, dim)


def kernel(
    inputs, x_weight, b_weight, dt_weight, dt_bias, decay_rate, conv_x, conv_b,
    query_c, query_gate, read_span, read_gain,
    cache, first_read,
    slab, wbuf, acc, proj, mixed, held, biasb, rateb, cxb, cbb, qb, gateb, gainb, rb,
    expand, sbuf, sendb, ybuf, redy, redz, reds, tot8,
    in_sem, load_sems, gsend, grecv, hsend, hrecv, asend, arecv,
    ysems, zsems, ssems, own_sem, stage,
):
    sp = lax.axis_index("sp")
    tp = lax.axis_index("tp")
    y = lax.rem(sp, NY)
    z = lax.div(sp, NY)
    core = lax.rem(tp, 2)
    partner = tp + 1 - 2 * core
    right = lax.rem(tp + 2, NTP)
    left = lax.rem(tp + NTP - 2, NTP)
    across = lax.rem(tp + NTP // 2, NTP)

    own_in = pltpu.make_async_copy(inputs, slab.at[tp, pl.ds(EDGE, TOK), :], in_sem)
    own_in.start()
    loads = [
        (x_weight, wbuf.at[:, pl.ds(0, XC)]),
        (b_weight, wbuf.at[:, pl.ds(XC, BC)]),
        (dt_weight, wbuf.at[:, pl.ds(CC, 128)]),
        (dt_bias, biasb),
        (decay_rate, rateb),
        (conv_x, cxb),
        (conv_b, cbb),
        (query_c, qb),
        (query_gate, gateb),
        (read_gain, gainb),
        (read_span, rb),
    ]
    copies = []
    for i, (src, dst) in enumerate(loads):
        c = pltpu.make_async_copy(src, dst, load_sems.at[i])
        c.start()
        copies.append(c)

    barrier = pltpu.get_barrier_semaphore()

    def at_y(other):
        return {"sp": z * NY + lax.rem(other, NY)}

    for i in range(1, NTP):
        pl.semaphore_signal(
            barrier, inc=1, device_id={"tp": lax.rem(tp + i, NTP)}, device_id_type=MESH
        )
    for i in range(1, NZ):
        pl.semaphore_signal(
            barrier, inc=1, device_id={"sp": lax.rem(z + i, NZ) * NY + y}, device_id_type=MESH
        )
    for side in (1, NY - 1):
        pl.semaphore_signal(barrier, inc=1, device_id=at_y(y + side), device_id_type=MESH)
    for side in (1, NSP - 1):
        pl.semaphore_signal(
            barrier, inc=1, device_id={"sp": lax.rem(sp + side, NSP)}, device_id_type=MESH
        )

    def tell(index, distance):
        for side in (distance, NY - distance):
            pl.semaphore_signal(
                stage.at[index], inc=1, device_id=at_y(y + side), device_id_type=MESH
            )

    @pl.when(sp == 0)
    def _():
        slab[tp, pl.ds(0, EDGE), :] = jnp.zeros((EDGE, FEAT), BF16)

    own_in.wait()
    pl.semaphore_wait(barrier, NTP - 1 + NZ - 1 + 4)
    tell(0, 1)

    def edge_in():
        return pltpu.make_async_remote_copy(
            src_ref=slab.at[tp, pl.ds(TOK, EDGE), :],
            dst_ref=slab.at[tp, pl.ds(0, EDGE), :],
            send_sem=hsend.at[0],
            recv_sem=hrecv.at[0],
            device_id={"sp": lax.rem(sp + 1, NSP)},
            device_id_type=MESH,
        )

    @pl.when(sp < NSP - 1)
    def _():
        edge_in().start()

    pieces = [(EDGE, ROWS_A), (0, EDGE), (TOP, ROWS_B)]

    def part(slot, j):
        return slab.at[slot, pl.ds(*pieces[j]), :]

    def forward(slot, j, dest):
        c = pltpu.make_async_remote_copy(
            src_ref=part(slot, j),
            dst_ref=part(slot, j),
            send_sem=gsend.at[j],
            recv_sem=grecv.at[slot, j],
            device_id={"tp": dest},
            device_id_type=MESH,
        )
        c.start()

    def arrive(slot, j):
        pltpu.make_async_remote_copy(
            src_ref=part(slot, j),
            dst_ref=part(slot, j),
            send_sem=gsend.at[j],
            recv_sem=grecv.at[slot, j],
            device_id={"tp": partner},
            device_id_type=MESH,
        ).wait_recv()

    def send_own(j):
        for dest in (across, right, left, partner):
            forward(tp, j, dest)

    ring = (right, left, across)

    def pass_on(j):
        for slot in ring:
            arrive(slot, j)
            forward(slot, j, partner)

    def twin(slot):
        return slot + 1 - 2 * core

    def product(slot, start, count):
        rows = pl.ds(pl.multiple_of(slot * FEAT, FEAT), FEAT)
        return jnp.dot(
            slab[slot, pl.ds(start, count), :], wbuf[rows, :], preferred_element_type=F32
        )

    def add(slot, start, count):
        acc[pl.ds(start, count), :] += product(slot, start, count)

    send_own(0)
    er = iota((256, 1024), 0) % 128
    ec = iota((256, 1024), 1)
    expand[...] = jnp.where(
        er == (ec // 512) * H + tp * 8 + (ec % 512) // P_SIZE, 1.0, 0.0
    ).astype(BF16)

    @pl.when(sp > 0)
    def _():
        edge_in().wait_recv()

    send_own(1)
    send_own(2)
    for c in copies:
        c.wait()
    acc[pl.ds(TOP, ROWS_B), :] = product(tp, TOP, ROWS_B)
    acc[pl.ds(0, TOP), :] = product(tp, 0, TOP)
    for j in (0, 1):
        arrive(partner, j)
    add(partner, 0, TOP)
    pass_on(0)
    pl.semaphore_wait(stage.at[0], 2)
    tell(1, 2)
    pass_on(1)
    for slot in ring:
        add(slot, 0, TOP)
    for slot in ring[:2]:
        for j in (0, 1):
            arrive(twin(slot), j)
        add(twin(slot), 0, TOP)
    pl.semaphore_wait(stage.at[1], 2)
    tell(2, 1)
    for j in (0, 1):
        arrive(twin(across), j)
    last = product(twin(across), 0, TOP)
    proj[pl.ds(0, TOP), :] = (acc[pl.ds(0, TOP), :CC] + last[:, :CC]).astype(BF16).astype(F32)
    acc[pl.ds(0, TOP), CC:] += last[:, CC:]

    @pl.when(sp == 0)
    def _():
        proj[pl.ds(0, EDGE), :] = jnp.zeros((EDGE, CC), F32)

    def edge_down():
        return pltpu.make_async_remote_copy(
            src_ref=proj.at[pl.ds(EDGE, 8), :],
            dst_ref=proj.at[pl.ds(EDGE + TOK, 8), :],
            send_sem=hsend.at[1],
            recv_sem=hrecv.at[1],
            device_id={"sp": lax.rem(sp + NSP - 1, NSP)},
            device_id_type=MESH,
        )

    @pl.when(sp > 0)
    def _():
        edge_down().start()

    bias = jnp.concatenate([biasb[0:1, :], biasb[1:2, :]], axis=1)
    rate = jnp.concatenate([rateb[0:1, :], rateb[1:2, :]], axis=1)
    row = iota((SPAN, SPAN), 0)
    col = iota((SPAN, SPAN), 1)
    later = jnp.where(col > row, 1.0, 0.0)
    earlier = jnp.where(col < row, 1.0, 0.0)

    def weights_of(k):
        dt_raw = acc[pl.ds(EDGE + k * SPAN, SPAN), CC:].astype(BF16).astype(F32)
        v = dt_raw + bias
        step = jnp.maximum(v, 0.0) + jnp.log1p(jnp.exp(-jnp.abs(v)))
        a = -(step * rate) / LEN
        tail = jnp.dot(later, a, precision=lax.Precision.HIGHEST, preferred_element_type=F32)
        head = jnp.dot(earlier, a, precision=lax.Precision.HIGHEST, preferred_element_type=F32)
        w = jnp.exp(jnp.where(col < H, tail, head)) * step
        redy[y, k : k + 1, pl.ds(512, 128)] = jnp.sum(a, axis=0, keepdims=True)
        high = w.astype(BF16)
        low = (w - high.astype(F32)).astype(BF16)
        return jnp.concatenate([high, low], axis=1)

    taps = [cxb[...].astype(F32), cbb[...].astype(F32)]

    def convolve(start, count):
        for block in range(CC // 256):
            tap = taps[0][:, block * 256 : (block + 1) * 256] if block < 2 else taps[1]
            cols = pl.ds(block * 256, 256)
            total = jnp.zeros((count, 256), F32)
            for o in range(KW):
                total = total + tap[o : o + 1] * proj[pl.ds(start + EDGE - 2 + o, count), cols]
            mixed[pl.ds(start, count), cols] = jax.nn.silu(total).astype(BF16)

    order = (4 * (row % 32) + row // 32 == col)
    order_t = jnp.where(order, 1.0, 0.0).astype(BF16)
    contract_last = (((1,), (1,)), ((), ()))
    queries = []
    for g in range(2):
        q8 = jnp.broadcast_to(qb[0, g : g + 1, :].astype(F32), (8, N)).astype(BF16)
        queries.append(
            lax.dot_general(q8, order_t, contract_last, preferred_element_type=F32).astype(BF16)
        )
    half = iota((32, 128), 1) < P_SIZE
    chosen = rb[0]

    def state_copy(k, d, s):
        return pltpu.make_async_remote_copy(
            src_ref=sendb.at[d, k],
            dst_ref=cache.at[2 * s + k],
            send_sem=asend,
            recv_sem=arecv,
            device_id={"sp": d},
            device_id_type=MESH,
        )

    across_y = [lax.rem(y + dy, NY) for dy in range(NY)]
    across_z = [lax.rem(z + dz, NZ) * NY for dz in range(NZ)]
    distances = (4, 5, 3, 6, 2, 7, 1)

    def send_states(k, first, last):
        for dy in distances[first:last]:
            for dz in range(NZ):
                state_copy(k, across_z[dz] + across_y[dy], sp).start()

    def send_column(k):
        for dz in range(1, NZ):
            state_copy(k, across_z[dz] + y, sp).start()

    own_out = []

    def states_of(k, pair):
        rows = pl.ds(k * SPAN, SPAN)
        keys_t = [
            lax.dot_general(
                order_t, mixed[rows, pl.ds(XC + g * N, N)], contract_last,
                preferred_element_type=F32,
            ).astype(BF16)
            for g in range(2)
        ]
        for e in range(2):
            wide = jnp.dot(pair, expand[:, pl.ds(e * 512, 512)], preferred_element_type=F32)
            weighted = (mixed[rows, pl.ds(0, XC)].astype(F32) * wide).astype(BF16)
            for g in range(2):
                state = jnp.dot(
                    keys_t[g], weighted[:, g * 256 : (g + 1) * 256], preferred_element_type=F32
                )
                read = jnp.dot(queries[g], state.astype(BF16), preferred_element_type=F32)
                ybuf[e : e + 1, pl.ds(g * 256, 256)] = read[0:1]
                held[e, g] = state
        at = jnp.full((1, 512), 2 * sp + k, jnp.int32)
        pick = jnp.full((1, 512), chosen, jnp.int32)
        redy[y, k : k + 1, pl.ds(0, 512)] = jnp.where(at <= pick, ybuf[0:1, :], 0.0) + jnp.where(
            at >= pick, ybuf[1:2, :], 0.0
        )

    def arrange(k):
        for e in range(2):
            for g in range(2):
                for j in range(2):
                    for a in range(2):
                        lanes = pl.ds(128 * j, 128)
                        one = held[e, g, pl.ds(64 * a, 32), lanes]
                        two = held[e, g, pl.ds(64 * a + 32, 32), lanes]
                        first = jnp.where(half, one, pltpu.roll(two, 64, 1))
                        second = jnp.where(half, pltpu.roll(one, 64, 1), two)
                        h = 4 * g + 2 * j
                        sbuf[a, pl.ds(h, 32, stride=8), :] = first
                        sbuf[a, pl.ds(h + 1, 32, stride=8), :] = second
            for a in range(2):
                sendb[:, k, e, :, pl.ds(a * 128, 128)] = (
                    sbuf[a].reshape(NSP, 8, 128).astype(BF16)
                )
        c = pltpu.make_async_copy(sendb.at[sp, k], cache.at[2 * sp + k], own_sem.at[k])
        c.start()
        own_out.append(c)

    pair = weights_of(0)
    for first in range(0, SPAN, 16):
        convolve(first, 16)
    pass_on(2)
    pl.semaphore_wait(stage.at[2], 2)
    states_of(0, pair)
    arrange(0)
    send_column(0)
    send_states(0, 0, EARLY)

    for slot in (partner, *ring, twin(right), twin(left)):
        if slot is not right and slot is not left and slot is not across:
            arrive(slot, 2)
        add(slot, TOP, ROWS_B)
    arrive(twin(across), 2)
    last = product(twin(across), TOP, ROWS_B)
    rest = pl.ds(TOP, ROWS_B)
    proj[rest, :] = (acc[rest, :CC] + last[:, :CC]).astype(BF16).astype(F32)
    acc[rest, CC:] += last[:, CC:]
    pair = weights_of(1)
    for first in range(SPAN, TOK - 16, 16):
        convolve(first, 16)

    @pl.when(sp < NSP - 1)
    def _():
        edge_down().wait_recv()

    @pl.when(sp == NSP - 1)
    def _():
        proj[pl.ds(EDGE + TOK, 8), :] = jnp.zeros((8, CC), F32)

    convolve(TOK - 16, 16)
    states_of(1, pair)

    def exchange(buffer, me, count, sems, place):
        for i in range(1, count):
            other = lax.rem(me + i, count)
            pltpu.make_async_remote_copy(
                src_ref=buffer.at[me],
                dst_ref=buffer.at[me],
                send_sem=sems.at[0],
                recv_sem=sems.at[1],
                device_id=place(other),
                device_id_type=MESH,
            ).start()

        return pltpu.make_async_remote_copy(
            src_ref=buffer.at[pl.ds(0, count - 1)],
            dst_ref=buffer.at[pl.ds(0, count - 1)],
            send_sem=sems.at[0],
            recv_sem=sems.at[1],
            device_id=place(me),
            device_id_type=MESH,
        )

    y_all = exchange(redy, y, NY, ysems, lambda d: {"sp": z * NY + d})
    send_states(0, EARLY, 7)
    arrange(1)
    send_column(1)
    send_states(1, 0, MID)

    def spread(rows):
        high = rows.astype(BF16)
        low = (rows - high.astype(F32)).astype(BF16)
        return jnp.dot(
            jnp.concatenate([high, low], axis=1),
            expand[:, pl.ds(0, 512)],
            preferred_element_type=F32,
        )

    gate = jax.nn.silu(gateb[0].astype(F32))
    y_all.wait_recv()
    base = 2 * NY * z
    ahead_lane = iota((8, 128), 1) < H
    block_log = jnp.zeros((8, 128), F32)
    span_logs = [jnp.zeros((8, 128), F32), jnp.zeros((8, 128), F32)]
    pick = jnp.full((8, 128), chosen, jnp.int32)
    span_at = [base + 2 * iota((8, 128), 0) + k for k in range(2)]
    for other in range(2 * NY):
        log = jnp.broadcast_to(
            redy[other // 2, other % 2 : other % 2 + 1, pl.ds(512, 128)], (8, 128)
        )
        here = jnp.full((8, 128), base + other, jnp.int32)
        log = jnp.where(ahead_lane, jnp.where(here <= pick, log, 0.0), jnp.where(here >= pick, log, 0.0))
        block_log = block_log + log
        for k in range(2):
            counted = jnp.where(
                ahead_lane,
                jnp.where(here > span_at[k], log, 0.0),
                jnp.where(here < span_at[k], log, 0.0),
            )
            span_logs[k] = span_logs[k] + counted
    span_weights = [jnp.exp(t + pltpu.roll(t, H, 1)) for t in span_logs]
    wide_weight = spread(jnp.concatenate(span_weights, axis=0))
    partial = jnp.zeros((8, 512), F32)
    for k in range(2):
        partial = partial + wide_weight[8 * k : 8 * k + 8] * redy[:, k, pl.ds(0, 512)]
    redz[z, :, pl.ds(0, 512)] = jnp.sum(partial, axis=0, keepdims=True)
    redz[z, :, pl.ds(512, 128)] = block_log[0:1]
    z_all = exchange(redz, z, NZ, zsems, lambda d: {"sp": d * NY + y})
    send_states(1, MID, 7)
    z_all.wait_recv()
    lane = iota((1, 128), 1)
    block_rows = []
    for block in range(NZ):
        after = jnp.zeros((1, 128), F32)
        before = jnp.zeros((1, 128), F32)
        for other in range(block + 1, NZ):
            after = after + redz[other, :, pl.ds(512, 128)]
        for other in range(block):
            before = before + redz[other, :, pl.ds(512, 128)]
        block_rows.append(jnp.where(lane < H, after, before))
    block_rows = block_rows + [jnp.zeros((8 - NZ, 128), F32)]
    logs = jnp.concatenate(block_rows, axis=0)
    block_factor = spread(jnp.exp(logs + pltpu.roll(logs, H, 1)))
    total = jnp.zeros((1, 512), F32)
    for block in range(NZ):
        total = total + block_factor[block : block + 1] * redz[block, :, pl.ds(0, 512)]
    for h in range(8):
        tot8[h : h + 1, :] = total[:, h * P_SIZE : (h + 1) * P_SIZE]
    gated = tot8[...] * gate
    squares = jnp.sum(jnp.sum(gated * gated, axis=0, keepdims=True), axis=1, keepdims=True)
    reds[tp] = jnp.broadcast_to(squares, (1, 128))
    s_all = exchange(reds, tp, NTP, ssems, lambda d: {"tp": d})
    s_all.wait_recv()
    square_sum = jnp.sum(reds[...], axis=0)[:, :64]
    scale = lax.rsqrt(square_sum / (H * P_SIZE) + EPSILON)
    first_read[0] = (gated * scale * gainb[...]).astype(BF16)

    for j, (start, count) in enumerate(pieces):
        sent = slab.at[pl.ds(0, NTP - 1), pl.ds(start, count), :]
        pltpu.make_async_remote_copy(
            src_ref=sent,
            dst_ref=sent,
            send_sem=gsend.at[j],
            recv_sem=gsend.at[j],
            device_id={"tp": partner},
            device_id_type=MESH,
        ).wait_send()

    @pl.when(sp < NSP - 1)
    def _():
        edge_in().wait_send()

    @pl.when(sp > 0)
    def _():
        edge_down().wait_send()

    y_all.wait_send()
    z_all.wait_send()
    s_all.wait_send()
    every = cache.at[pl.ds(0, 2 * NSP - 2)]
    states = pltpu.make_async_remote_copy(
        src_ref=every,
        dst_ref=every,
        send_sem=asend,
        recv_sem=arecv,
        device_id={"sp": sp},
        device_id_type=MESH,
    )
    states.wait_recv()
    states.wait_send()
    for c in own_out:
        c.wait()


def write_out(cache, first_read, cache_out, first_out, sems):
    copies = [
        pltpu.make_async_copy(
            cache.at[pl.ds(16 * i, 16)], cache_out.at[pl.ds(16 * i, 16)], sems.at[i]
        )
        for i in range(4)
    ]
    copies.append(pltpu.make_async_copy(first_read, first_out, sems.at[4]))
    for c in copies:
        c.start()
    for c in copies:
        c.wait()


def per_device(*args):
    dma = pltpu.SemaphoreType.DMA
    any_spec = pl.BlockSpec(memory_space=pl.ANY)
    vmem_spec = pl.BlockSpec(memory_space=pltpu.VMEM)
    shapes = (
        jax.ShapeDtypeStruct((64, 2, 8, 256), BF16),
        jax.ShapeDtypeStruct((1, 8, 64), BF16),
    )
    results = pl.pallas_call(
        kernel,
        out_shape=tuple(pltpu.VMEM(t.shape, t.dtype) for t in shapes),
        in_specs=[any_spec] * 12,
        out_specs=(vmem_spec, vmem_spec),
        scratch_shapes=[
            pltpu.VMEM((NTP, EDGE + TOK, FEAT), BF16),
            pltpu.VMEM((2048, WC), BF16),
            pltpu.VMEM((EDGE + TOK, WC), F32),
            pltpu.VMEM((EDGE + TOK + 8, CC), F32),
            pltpu.VMEM((TOK, CC), BF16),
            pltpu.VMEM((2, 2, N, 256), F32),
            pltpu.VMEM((2, H), F32),
            pltpu.VMEM((2, H), F32),
            pltpu.VMEM((KW, XC), BF16),
            pltpu.VMEM((KW, BC), BF16),
            pltpu.VMEM((1, 2, N), BF16),
            pltpu.VMEM((1, 8, P_SIZE), BF16),
            pltpu.VMEM((8, P_SIZE), F32),
            pltpu.SMEM((1,), jnp.int32),
            pltpu.VMEM((256, 1024), BF16),
            pltpu.VMEM((2, 256, 128), F32),
            pltpu.VMEM((NSP, 2, 2, 8, 256), BF16),
            pltpu.VMEM((8, 512), F32),
            pltpu.VMEM((NY, 2, 640), F32),
            pltpu.VMEM((NZ, 1, 640), F32),
            pltpu.VMEM((NTP, 1, 128), F32),
            pltpu.VMEM((8, P_SIZE), F32),
            dma,
            dma((11,)),
            dma((3,)),
            dma((NTP, 3)),
            dma((2,)),
            dma((2,)),
            dma,
            dma,
            dma((2,)),
            dma((2,)),
            dma((2,)),
            dma((2,)),
            pltpu.SemaphoreType.REGULAR((3,)),
        ],
        compiler_params=pltpu.CompilerParams(collective_id=0, has_side_effects=True),
    )(*args)
    results = [pltpu.with_memory_space_constraint(r, pltpu.VMEM) for r in results]
    return pl.pallas_call(
        write_out,
        out_shape=shapes,
        in_specs=[vmem_spec] * 2,
        out_specs=(any_spec, any_spec),
        scratch_shapes=[dma((5,))],
    )(*results)


def solution(mesh):
    return jax.shard_map(
        per_device,
        mesh=mesh,
        in_specs=(
            P(("gr", "sp"), "tp"),
            P(None, "tp"),
            P(None, "tp"),
            P(),
            P(),
            P(),
            P(None, "tp"),
            P(None, "tp"),
            P("gr", "tp", None),
            P("gr", "tp", None),
            P("gr"),
            P("tp", None),
        ),
        out_specs=(P("gr", None, "tp", "sp"), P("gr", "tp", None)),
        check_vma=False,
    )
```

```python
import jax
import jax.numpy as jnp
from jax import lax
from jax.experimental import pallas as pl
from jax.experimental.pallas import tpu as pltpu
from jax.sharding import PartitionSpec as P

H = 64
P_SIZE = 64
G = 16
N = 128
KW = 5
SPAN = 128
EPSILON = 1e-06
LEN = 8192
NY = 8
NZ = 4
NX = 4
NSP = 32
NTP = 8
TOK = 256
FEAT = 256
XC = 512
BC = 256
CC = 768
WC = 896
EDGE = 16
ROWS_A = 144
ROWS_B = TOK - ROWS_A
TOP = EDGE + ROWS_A
EARLY = 2
MID = 0

MESH = pl.DeviceIdType.MESH
F32 = jnp.float32
BF16 = jnp.bfloat16


def iota(shape, dim):
    return lax.broadcasted_iota(jnp.int32, shape, dim)


def kernel(
    inputs, x_weight, b_weight, dt_weight, dt_bias, decay_rate, conv_x, conv_b,
    query_c, query_gate, read_span, read_gain,
    cache, first_read,
    slab, wbuf, acc, proj, mixed, held, biasb, rateb, cxb, cbb, qb, gateb, gainb, rb,
    expand, sbuf, sendb, ybuf, redy, redz, reds, tot8,
    in_sem, load_sems, gsend, grecv, hsend, hrecv, asend, arecv,
    ysems, zsems, ssems, own_sem, stage,
):
    sp = lax.axis_index("sp")
    tp = lax.axis_index("tp")
    y = lax.rem(sp, NY)
    z = lax.div(sp, NY)
    core = lax.rem(tp, 2)
    partner = tp + 1 - 2 * core
    right = lax.rem(tp + 2, NTP)
    left = lax.rem(tp + NTP - 2, NTP)
    across = lax.rem(tp + NTP // 2, NTP)

    own_in = pltpu.make_async_copy(inputs, slab.at[tp, pl.ds(EDGE, TOK), :], in_sem)
    own_in.start()
    loads = []
    for width, weight, first, cuts in (
        (XC, x_weight, 0, 4), (BC, b_weight, XC, 2), (128, dt_weight, CC, 1)
    ):
        for i in range(cuts):
            depth = pl.ds(i * (2048 // cuts), 2048 // cuts)
            loads.append((weight.at[depth, :], wbuf.at[depth, pl.ds(first, width)]))
    loads += [
        (dt_bias, biasb),
        (decay_rate, rateb),
        (conv_x, cxb),
        (conv_b, cbb),
        (query_c, qb),
        (query_gate, gateb),
        (read_gain, gainb),
        (read_span, rb),
    ]
    copies = []
    for i, (src, dst) in enumerate(loads):
        c = pltpu.make_async_copy(src, dst, load_sems.at[i])
        c.start(priority=1)
        copies.append(c)

    barrier = pltpu.get_barrier_semaphore()

    def at_y(other):
        return {"sp": z * NY + lax.rem(other, NY)}

    for i in range(1, NTP):
        pl.semaphore_signal(
            barrier, inc=1, device_id={"tp": lax.rem(tp + i, NTP)}, device_id_type=MESH
        )
    for i in range(1, NZ):
        pl.semaphore_signal(
            barrier, inc=1, device_id={"sp": lax.rem(z + i, NZ) * NY + y}, device_id_type=MESH
        )
    for side in (1, NY - 1):
        pl.semaphore_signal(barrier, inc=1, device_id=at_y(y + side), device_id_type=MESH)
    for side in (1, NSP - 1):
        pl.semaphore_signal(
            barrier, inc=1, device_id={"sp": lax.rem(sp + side, NSP)}, device_id_type=MESH
        )

    def tell(index, distance):
        for side in (distance, NY - distance):
            pl.semaphore_signal(
                stage.at[index], inc=1, device_id=at_y(y + side), device_id_type=MESH
            )

    @pl.when(sp == 0)
    def _():
        slab[tp, pl.ds(0, EDGE), :] = jnp.zeros((EDGE, FEAT), BF16)

    own_in.wait()
    pl.semaphore_wait(barrier, NTP - 1 + NZ - 1 + 4)
    tell(0, 1)

    def edge_in():
        return pltpu.make_async_remote_copy(
            src_ref=slab.at[tp, pl.ds(TOK, EDGE), :],
            dst_ref=slab.at[tp, pl.ds(0, EDGE), :],
            send_sem=hsend.at[0],
            recv_sem=hrecv.at[0],
            device_id={"sp": lax.rem(sp + 1, NSP)},
            device_id_type=MESH,
        )

    @pl.when(sp < NSP - 1)
    def _():
        edge_in().start()

    pieces = [(EDGE, ROWS_A), (0, EDGE), (TOP, ROWS_B)]

    def part(slot, j):
        return slab.at[slot, pl.ds(*pieces[j]), :]

    def forward(slot, j, dest):
        c = pltpu.make_async_remote_copy(
            src_ref=part(slot, j),
            dst_ref=part(slot, j),
            send_sem=gsend.at[j],
            recv_sem=grecv.at[slot, j],
            device_id={"tp": dest},
            device_id_type=MESH,
        )
        c.start()

    def arrive(slot, j):
        pltpu.make_async_remote_copy(
            src_ref=part(slot, j),
            dst_ref=part(slot, j),
            send_sem=gsend.at[j],
            recv_sem=grecv.at[slot, j],
            device_id={"tp": partner},
            device_id_type=MESH,
        ).wait_recv()

    def send_own(j):
        for dest in (across, right, left, partner):
            forward(tp, j, dest)

    ring = (right, left, across)

    def pass_on(j):
        for slot in ring:
            arrive(slot, j)
            forward(slot, j, partner)

    def twin(slot):
        return slot + 1 - 2 * core

    def product(slot, start, count):
        rows = pl.ds(pl.multiple_of(slot * FEAT, FEAT), FEAT)
        return jnp.dot(
            slab[slot, pl.ds(start, count), :], wbuf[rows, :], preferred_element_type=F32
        )

    def add(slot, start, count):
        acc[pl.ds(start, count), :] += product(slot, start, count)

    send_own(0)
    er = iota((256, 1024), 0) % 128
    ec = iota((256, 1024), 1)
    expand[...] = jnp.where(
        er == (ec // 512) * H + tp * 8 + (ec % 512) // P_SIZE, 1.0, 0.0
    ).astype(BF16)

    @pl.when(sp > 0)
    def _():
        edge_in().wait_recv()

    send_own(1)
    send_own(2)
    for c in copies:
        c.wait()
    acc[pl.ds(TOP, ROWS_B), :] = product(tp, TOP, ROWS_B)
    acc[pl.ds(0, TOP), :] = product(tp, 0, TOP)
    for j in (0, 1):
        arrive(partner, j)
    add(partner, 0, TOP)
    pass_on(0)
    pl.semaphore_wait(stage.at[0], 2)
    tell(1, 2)
    pass_on(1)
    for slot in ring:
        add(slot, 0, TOP)
    for slot in ring[:2]:
        for j in (0, 1):
            arrive(twin(slot), j)
        add(twin(slot), 0, TOP)
    pl.semaphore_wait(stage.at[1], 2)
    tell(2, 1)
    for j in (0, 1):
        arrive(twin(across), j)
    last = product(twin(across), 0, TOP)
    proj[pl.ds(0, TOP), :] = (acc[pl.ds(0, TOP), :CC] + last[:, :CC]).astype(BF16).astype(F32)
    acc[pl.ds(0, TOP), CC:] += last[:, CC:]

    @pl.when(sp == 0)
    def _():
        proj[pl.ds(0, EDGE), :] = jnp.zeros((EDGE, CC), F32)

    def edge_down():
        return pltpu.make_async_remote_copy(
            src_ref=proj.at[pl.ds(EDGE, 8), :],
            dst_ref=proj.at[pl.ds(EDGE + TOK, 8), :],
            send_sem=hsend.at[1],
            recv_sem=hrecv.at[1],
            device_id={"sp": lax.rem(sp + NSP - 1, NSP)},
            device_id_type=MESH,
        )

    @pl.when(sp > 0)
    def _():
        edge_down().start()

    bias = jnp.concatenate([biasb[0:1, :], biasb[1:2, :]], axis=1)
    rate = jnp.concatenate([rateb[0:1, :], rateb[1:2, :]], axis=1)
    row = iota((SPAN, SPAN), 0)
    col = iota((SPAN, SPAN), 1)
    later = jnp.where(col > row, 1.0, 0.0)
    earlier = jnp.where(col < row, 1.0, 0.0)

    def weights_of(k):
        dt_raw = acc[pl.ds(EDGE + k * SPAN, SPAN), CC:].astype(BF16).astype(F32)
        v = dt_raw + bias
        step = jnp.maximum(v, 0.0) + jnp.log1p(jnp.exp(-jnp.abs(v)))
        a = -(step * rate) / LEN
        tail = jnp.dot(later, a, precision=lax.Precision.HIGHEST, preferred_element_type=F32)
        head = jnp.dot(earlier, a, precision=lax.Precision.HIGHEST, preferred_element_type=F32)
        w = jnp.exp(jnp.where(col < H, tail, head)) * step
        redy[y, k : k + 1, pl.ds(512, 128)] = jnp.sum(a, axis=0, keepdims=True)
        high = w.astype(BF16)
        low = (w - high.astype(F32)).astype(BF16)
        return jnp.concatenate([high, low], axis=1)

    taps = [cxb[...].astype(F32), cbb[...].astype(F32)]

    def convolve(start, count):
        for block in range(CC // 256):
            tap = taps[0][:, block * 256 : (block + 1) * 256] if block < 2 else taps[1]
            cols = pl.ds(block * 256, 256)
            total = jnp.zeros((count, 256), F32)
            for o in range(KW):
                total = total + tap[o : o + 1] * proj[pl.ds(start + EDGE - 2 + o, count), cols]
            mixed[pl.ds(start, count), cols] = jax.nn.silu(total).astype(BF16)

    order = (4 * (row % 32) + row // 32 == col)
    order_t = jnp.where(order, 1.0, 0.0).astype(BF16)
    contract_last = (((1,), (1,)), ((), ()))
    queries = []
    for g in range(2):
        q8 = jnp.broadcast_to(qb[0, g : g + 1, :].astype(F32), (8, N)).astype(BF16)
        queries.append(
            lax.dot_general(q8, order_t, contract_last, preferred_element_type=F32).astype(BF16)
        )
    half = iota((32, 128), 1) < P_SIZE
    chosen = rb[0]

    def state_copy(k, d, s):
        return pltpu.make_async_remote_copy(
            src_ref=sendb.at[d, k],
            dst_ref=cache.at[2 * s + k],
            send_sem=asend,
            recv_sem=arecv,
            device_id={"sp": d},
            device_id_type=MESH,
        )

    across_y = [lax.rem(y + dy, NY) for dy in range(NY)]
    across_z = [lax.rem(z + dz, NZ) * NY for dz in range(NZ)]
    distances = (4, 5, 3, 6, 2, 7, 1)

    def send_states(k, first, last):
        for dy in distances[first:last]:
            for dz in range(NZ):
                state_copy(k, across_z[dz] + across_y[dy], sp).start()

    def send_column(k):
        for dz in range(1, NZ):
            state_copy(k, across_z[dz] + y, sp).start()

    own_out = []

    def states_of(k, pair):
        rows = pl.ds(k * SPAN, SPAN)
        keys_t = [
            lax.dot_general(
                order_t, mixed[rows, pl.ds(XC + g * N, N)], contract_last,
                preferred_element_type=F32,
            ).astype(BF16)
            for g in range(2)
        ]
        for e in range(2):
            wide = jnp.dot(pair, expand[:, pl.ds(e * 512, 512)], preferred_element_type=F32)
            weighted = (mixed[rows, pl.ds(0, XC)].astype(F32) * wide).astype(BF16)
            for g in range(2):
                state = jnp.dot(
                    keys_t[g], weighted[:, g * 256 : (g + 1) * 256], preferred_element_type=F32
                )
                read = jnp.dot(queries[g], state.astype(BF16), preferred_element_type=F32)
                ybuf[e : e + 1, pl.ds(g * 256, 256)] = read[0:1]
                held[e, g] = state
        at = jnp.full((1, 512), 2 * sp + k, jnp.int32)
        pick = jnp.full((1, 512), chosen, jnp.int32)
        redy[y, k : k + 1, pl.ds(0, 512)] = jnp.where(at <= pick, ybuf[0:1, :], 0.0) + jnp.where(
            at >= pick, ybuf[1:2, :], 0.0
        )

    def arrange(k):
        for e in range(2):
            for g in range(2):
                for j in range(2):
                    for a in range(2):
                        lanes = pl.ds(128 * j, 128)
                        one = held[e, g, pl.ds(64 * a, 32), lanes]
                        two = held[e, g, pl.ds(64 * a + 32, 32), lanes]
                        first = jnp.where(half, one, pltpu.roll(two, 64, 1))
                        second = jnp.where(half, pltpu.roll(one, 64, 1), two)
                        h = 4 * g + 2 * j
                        sbuf[a, pl.ds(h, 32, stride=8), :] = first
                        sbuf[a, pl.ds(h + 1, 32, stride=8), :] = second
            for a in range(2):
                sendb[:, k, e, :, pl.ds(a * 128, 128)] = (
                    sbuf[a].reshape(NSP, 8, 128).astype(BF16)
                )
        c = pltpu.make_async_copy(sendb.at[sp, k], cache.at[2 * sp + k], own_sem.at[k])
        c.start()
        own_out.append(c)

    pair = weights_of(0)
    for first in range(0, SPAN, 16):
        convolve(first, 16)
    pass_on(2)
    pl.semaphore_wait(stage.at[2], 2)
    states_of(0, pair)
    arrange(0)
    send_column(0)
    send_states(0, 0, EARLY)

    for slot in (partner, *ring, twin(right), twin(left)):
        if slot is not right and slot is not left and slot is not across:
            arrive(slot, 2)
        add(slot, TOP, ROWS_B)
    arrive(twin(across), 2)
    last = product(twin(across), TOP, ROWS_B)
    rest = pl.ds(TOP, ROWS_B)
    proj[rest, :] = (acc[rest, :CC] + last[:, :CC]).astype(BF16).astype(F32)
    acc[rest, CC:] += last[:, CC:]
    pair = weights_of(1)
    for first in range(SPAN, TOK - 16, 16):
        convolve(first, 16)

    @pl.when(sp < NSP - 1)
    def _():
        edge_down().wait_recv()

    @pl.when(sp == NSP - 1)
    def _():
        proj[pl.ds(EDGE + TOK, 8), :] = jnp.zeros((8, CC), F32)

    convolve(TOK - 16, 16)
    states_of(1, pair)

    def exchange(buffer, me, count, sems, place):
        for i in range(1, count):
            other = lax.rem(me + i, count)
            pltpu.make_async_remote_copy(
                src_ref=buffer.at[me],
                dst_ref=buffer.at[me],
                send_sem=sems.at[0],
                recv_sem=sems.at[1],
                device_id=place(other),
                device_id_type=MESH,
            ).start()

        return pltpu.make_async_remote_copy(
            src_ref=buffer.at[pl.ds(0, count - 1)],
            dst_ref=buffer.at[pl.ds(0, count - 1)],
            send_sem=sems.at[0],
            recv_sem=sems.at[1],
            device_id=place(me),
            device_id_type=MESH,
        )

    y_all = exchange(redy, y, NY, ysems, lambda d: {"sp": z * NY + d})
    send_states(0, EARLY, 7)
    arrange(1)
    send_column(1)
    send_states(1, 0, MID)

    def spread(rows):
        high = rows.astype(BF16)
        low = (rows - high.astype(F32)).astype(BF16)
        return jnp.dot(
            jnp.concatenate([high, low], axis=1),
            expand[:, pl.ds(0, 512)],
            preferred_element_type=F32,
        )

    gate = jax.nn.silu(gateb[0].astype(F32))
    y_all.wait_recv()
    base = 2 * NY * z
    ahead_lane = iota((8, 128), 1) < H
    block_log = jnp.zeros((8, 128), F32)
    span_logs = [jnp.zeros((8, 128), F32), jnp.zeros((8, 128), F32)]
    pick = jnp.full((8, 128), chosen, jnp.int32)
    span_at = [base + 2 * iota((8, 128), 0) + k for k in range(2)]
    for other in range(2 * NY):
        log = jnp.broadcast_to(
            redy[other // 2, other % 2 : other % 2 + 1, pl.ds(512, 128)], (8, 128)
        )
        here = jnp.full((8, 128), base + other, jnp.int32)
        log = jnp.where(ahead_lane, jnp.where(here <= pick, log, 0.0), jnp.where(here >= pick, log, 0.0))
        block_log = block_log + log
        for k in range(2):
            counted = jnp.where(
                ahead_lane,
                jnp.where(here > span_at[k], log, 0.0),
                jnp.where(here < span_at[k], log, 0.0),
            )
            span_logs[k] = span_logs[k] + counted
    span_weights = [jnp.exp(t + pltpu.roll(t, H, 1)) for t in span_logs]
    wide_weight = spread(jnp.concatenate(span_weights, axis=0))
    partial = jnp.zeros((8, 512), F32)
    for k in range(2):
        partial = partial + wide_weight[8 * k : 8 * k + 8] * redy[:, k, pl.ds(0, 512)]
    redz[z, :, pl.ds(0, 512)] = jnp.sum(partial, axis=0, keepdims=True)
    redz[z, :, pl.ds(512, 128)] = block_log[0:1]
    z_all = exchange(redz, z, NZ, zsems, lambda d: {"sp": d * NY + y})
    send_states(1, MID, 7)
    z_all.wait_recv()
    lane = iota((1, 128), 1)
    block_rows = []
    for block in range(NZ):
        after = jnp.zeros((1, 128), F32)
        before = jnp.zeros((1, 128), F32)
        for other in range(block + 1, NZ):
            after = after + redz[other, :, pl.ds(512, 128)]
        for other in range(block):
            before = before + redz[other, :, pl.ds(512, 128)]
        block_rows.append(jnp.where(lane < H, after, before))
    block_rows = block_rows + [jnp.zeros((8 - NZ, 128), F32)]
    logs = jnp.concatenate(block_rows, axis=0)
    block_factor = spread(jnp.exp(logs + pltpu.roll(logs, H, 1)))
    total = jnp.zeros((1, 512), F32)
    for block in range(NZ):
        total = total + block_factor[block : block + 1] * redz[block, :, pl.ds(0, 512)]
    for h in range(8):
        tot8[h : h + 1, :] = total[:, h * P_SIZE : (h + 1) * P_SIZE]
    gated = tot8[...] * gate
    squares = jnp.sum(jnp.sum(gated * gated, axis=0, keepdims=True), axis=1, keepdims=True)
    reds[tp] = jnp.broadcast_to(squares, (1, 128))
    s_all = exchange(reds, tp, NTP, ssems, lambda d: {"tp": d})
    s_all.wait_recv()
    square_sum = jnp.sum(reds[...], axis=0)[:, :64]
    scale = lax.rsqrt(square_sum / (H * P_SIZE) + EPSILON)
    first_read[0] = (gated * scale * gainb[...]).astype(BF16)

    for j, (start, count) in enumerate(pieces):
        sent = slab.at[pl.ds(0, NTP - 1), pl.ds(start, count), :]
        pltpu.make_async_remote_copy(
            src_ref=sent,
            dst_ref=sent,
            send_sem=gsend.at[j],
            recv_sem=gsend.at[j],
            device_id={"tp": partner},
            device_id_type=MESH,
        ).wait_send()

    @pl.when(sp < NSP - 1)
    def _():
        edge_in().wait_send()

    @pl.when(sp > 0)
    def _():
        edge_down().wait_send()

    y_all.wait_send()
    z_all.wait_send()
    s_all.wait_send()
    every = cache.at[pl.ds(0, 2 * NSP - 2)]
    states = pltpu.make_async_remote_copy(
        src_ref=every,
        dst_ref=every,
        send_sem=asend,
        recv_sem=arecv,
        device_id={"sp": sp},
        device_id_type=MESH,
    )
    states.wait_recv()
    states.wait_send()
    for c in own_out:
        c.wait()


def write_out(cache, first_read, cache_out, first_out, sems):
    copies = [
        pltpu.make_async_copy(
            cache.at[pl.ds(16 * i, 16)], cache_out.at[pl.ds(16 * i, 16)], sems.at[i]
        )
        for i in range(4)
    ]
    copies.append(pltpu.make_async_copy(first_read, first_out, sems.at[4]))
    for c in copies:
        c.start()
    for c in copies:
        c.wait()


def per_device(*args):
    dma = pltpu.SemaphoreType.DMA
    any_spec = pl.BlockSpec(memory_space=pl.ANY)
    vmem_spec = pl.BlockSpec(memory_space=pltpu.VMEM)
    shapes = (
        jax.ShapeDtypeStruct((64, 2, 8, 256), BF16),
        jax.ShapeDtypeStruct((1, 8, 64), BF16),
    )
    results = pl.pallas_call(
        kernel,
        out_shape=tuple(pltpu.VMEM(t.shape, t.dtype) for t in shapes),
        in_specs=[any_spec] * 12,
        out_specs=(vmem_spec, vmem_spec),
        scratch_shapes=[
            pltpu.VMEM((NTP, EDGE + TOK, FEAT), BF16),
            pltpu.VMEM((2048, WC), BF16),
            pltpu.VMEM((EDGE + TOK, WC), F32),
            pltpu.VMEM((EDGE + TOK + 8, CC), F32),
            pltpu.VMEM((TOK, CC), BF16),
            pltpu.VMEM((2, 2, N, 256), F32),
            pltpu.VMEM((2, H), F32),
            pltpu.VMEM((2, H), F32),
            pltpu.VMEM((KW, XC), BF16),
            pltpu.VMEM((KW, BC), BF16),
            pltpu.VMEM((1, 2, N), BF16),
            pltpu.VMEM((1, 8, P_SIZE), BF16),
            pltpu.VMEM((8, P_SIZE), F32),
            pltpu.SMEM((1,), jnp.int32),
            pltpu.VMEM((256, 1024), BF16),
            pltpu.VMEM((2, 256, 128), F32),
            pltpu.VMEM((NSP, 2, 2, 8, 256), BF16),
            pltpu.VMEM((8, 512), F32),
            pltpu.VMEM((NY, 2, 640), F32),
            pltpu.VMEM((NZ, 1, 640), F32),
            pltpu.VMEM((NTP, 1, 128), F32),
            pltpu.VMEM((8, P_SIZE), F32),
            dma,
            dma((15,)),
            dma((3,)),
            dma((NTP, 3)),
            dma((2,)),
            dma((2,)),
            dma,
            dma,
            dma((2,)),
            dma((2,)),
            dma((2,)),
            dma((2,)),
            pltpu.SemaphoreType.REGULAR((3,)),
        ],
        compiler_params=pltpu.CompilerParams(collective_id=0, has_side_effects=True),
    )(*args)
    results = [pltpu.with_memory_space_constraint(r, pltpu.VMEM) for r in results]
    return pl.pallas_call(
        write_out,
        out_shape=shapes,
        in_specs=[vmem_spec] * 2,
        out_specs=(any_spec, any_spec),
        scratch_shapes=[dma((5,))],
    )(*results)


def solution(mesh):
    return jax.shard_map(
        per_device,
        mesh=mesh,
        in_specs=(
            P(("gr", "sp"), "tp"),
            P(None, "tp"),
            P(None, "tp"),
            P(),
            P(),
            P(),
            P(None, "tp"),
            P(None, "tp"),
            P("gr", "tp", None),
            P("gr", "tp", None),
            P("gr"),
            P("tp", None),
        ),
        out_specs=(P("gr", None, "tp", "sp"), P("gr", "tp", None)),
        check_vma=False,
    )
```

```python
import jax
import jax.numpy as jnp
from jax import lax
from jax.experimental import pallas as pl
from jax.experimental.pallas import tpu as pltpu
from jax.sharding import PartitionSpec as P

H = 64
P_SIZE = 64
G = 16
N = 128
KW = 5
SPAN = 128
EPSILON = 1e-06
LEN = 8192
NY = 8
NZ = 4
NX = 4
NSP = 32
NTP = 8
TOK = 256
FEAT = 256
XC = 512
BC = 256
CC = 768
WC = 896
EDGE = 16
ROWS_A = 144
ROWS_B = TOK - ROWS_A
TOP = EDGE + ROWS_A
EARLY = 2
MID = 0

MESH = pl.DeviceIdType.MESH
F32 = jnp.float32
BF16 = jnp.bfloat16


def iota(shape, dim):
    return lax.broadcasted_iota(jnp.int32, shape, dim)


def kernel(
    inputs, x_weight, b_weight, dt_weight, dt_bias, decay_rate, conv_x, conv_b,
    query_c, query_gate, read_span, read_gain,
    cache, first_read,
    slab, wbuf, acc, proj, mixed, held, biasb, rateb, cxb, cbb, qb, gateb, gainb, rb,
    expand, sbuf, sendb, ybuf, redy, redz, reds, tot8,
    in_sem, load_sems, gsend, grecv, hsend, hrecv, asend, arecv,
    ysems, zsems, ssems, own_sem, stage,
):
    sp = lax.axis_index("sp")
    tp = lax.axis_index("tp")
    y = lax.rem(sp, NY)
    z = lax.div(sp, NY)
    core = lax.rem(tp, 2)
    partner = tp + 1 - 2 * core
    right = lax.rem(tp + 2, NTP)
    left = lax.rem(tp + NTP - 2, NTP)
    across = lax.rem(tp + NTP // 2, NTP)

    own_in = pltpu.make_async_copy(inputs, slab.at[tp, pl.ds(EDGE, TOK), :], in_sem)
    own_in.start()
    loads = []
    for width, weight, first, cuts in (
        (XC, x_weight, 0, 4), (BC, b_weight, XC, 2), (128, dt_weight, CC, 1)
    ):
        for i in range(cuts):
            depth = pl.ds(i * (2048 // cuts), 2048 // cuts)
            loads.append((weight.at[depth, :], wbuf.at[depth, pl.ds(first, width)]))
    loads += [
        (dt_bias, biasb),
        (decay_rate, rateb),
        (conv_x, cxb),
        (conv_b, cbb),
        (query_c, qb),
        (query_gate, gateb),
        (read_gain, gainb),
        (read_span, rb),
    ]
    copies = []
    for i, (src, dst) in enumerate(loads):
        c = pltpu.make_async_copy(src, dst, load_sems.at[i])
        c.start(priority=1)
        copies.append(c)

    barrier = pltpu.get_barrier_semaphore()

    def at_y(other):
        return {"sp": z * NY + lax.rem(other, NY)}

    for i in range(1, NTP):
        pl.semaphore_signal(
            barrier, inc=1, device_id={"tp": lax.rem(tp + i, NTP)}, device_id_type=MESH
        )
    for i in range(1, NZ):
        pl.semaphore_signal(
            barrier, inc=1, device_id={"sp": lax.rem(z + i, NZ) * NY + y}, device_id_type=MESH
        )
    for side in (1, NY - 1):
        pl.semaphore_signal(barrier, inc=1, device_id=at_y(y + side), device_id_type=MESH)
    for side in (1, NSP - 1):
        pl.semaphore_signal(
            barrier, inc=1, device_id={"sp": lax.rem(sp + side, NSP)}, device_id_type=MESH
        )

    def tell(index, distance):
        for side in (distance, NY - distance):
            pl.semaphore_signal(
                stage.at[index], inc=1, device_id=at_y(y + side), device_id_type=MESH
            )

    @pl.when(sp == 0)
    def _():
        slab[tp, pl.ds(0, EDGE), :] = jnp.zeros((EDGE, FEAT), BF16)

    own_in.wait()
    pl.semaphore_wait(barrier, NTP - 1 + NZ - 1 + 4)
    tell(0, 1)

    def edge_in():
        return pltpu.make_async_remote_copy(
            src_ref=slab.at[tp, pl.ds(TOK, EDGE), :],
            dst_ref=slab.at[tp, pl.ds(0, EDGE), :],
            send_sem=hsend.at[0],
            recv_sem=hrecv.at[0],
            device_id={"sp": lax.rem(sp + 1, NSP)},
            device_id_type=MESH,
        )

    @pl.when(sp < NSP - 1)
    def _():
        edge_in().start()

    pieces = [(EDGE, ROWS_A), (0, EDGE), (TOP, ROWS_B)]

    def part(slot, j):
        return slab.at[slot, pl.ds(*pieces[j]), :]

    def forward(slot, j, dest):
        c = pltpu.make_async_remote_copy(
            src_ref=part(slot, j),
            dst_ref=part(slot, j),
            send_sem=gsend.at[j],
            recv_sem=grecv.at[slot, j],
            device_id={"tp": dest},
            device_id_type=MESH,
        )
        c.start()

    def arrive(slot, j):
        pltpu.make_async_remote_copy(
            src_ref=part(slot, j),
            dst_ref=part(slot, j),
            send_sem=gsend.at[j],
            recv_sem=grecv.at[slot, j],
            device_id={"tp": partner},
            device_id_type=MESH,
        ).wait_recv()

    def send_own(j):
        for dest in (across, right, left, partner):
            forward(tp, j, dest)

    ring = (right, left, across)

    def pass_on(j):
        for slot in ring:
            arrive(slot, j)
            forward(slot, j, partner)

    def twin(slot):
        return slot + 1 - 2 * core

    def product(slot, start, count):
        rows = pl.ds(pl.multiple_of(slot * FEAT, FEAT), FEAT)
        return jnp.dot(
            slab[slot, pl.ds(start, count), :], wbuf[rows, :], preferred_element_type=F32
        )

    def add(slot, start, count):
        acc[pl.ds(start, count), :] += product(slot, start, count)

    send_own(0)
    er = iota((256, 1024), 0) % 128
    ec = iota((256, 1024), 1)
    expand[...] = jnp.where(
        er == (ec // 512) * H + tp * 8 + (ec % 512) // P_SIZE, 1.0, 0.0
    ).astype(BF16)

    @pl.when(sp > 0)
    def _():
        edge_in().wait_recv()

    send_own(1)
    send_own(2)
    for c in copies:
        c.wait()
    acc[pl.ds(TOP, ROWS_B), :] = product(tp, TOP, ROWS_B)
    acc[pl.ds(0, TOP), :] = product(tp, 0, TOP)
    for j in (0, 1):
        arrive(partner, j)
    add(partner, 0, TOP)
    pass_on(0)
    pl.semaphore_wait(stage.at[0], 2)
    tell(1, 2)
    pass_on(1)
    for slot in ring:
        add(slot, 0, TOP)
    for slot in ring[:2]:
        for j in (0, 1):
            arrive(twin(slot), j)
        add(twin(slot), 0, TOP)
    pl.semaphore_wait(stage.at[1], 2)
    tell(2, 1)
    for j in (0, 1):
        arrive(twin(across), j)
    last = product(twin(across), 0, TOP)
    proj[pl.ds(0, TOP), :] = (acc[pl.ds(0, TOP), :CC] + last[:, :CC]).astype(BF16).astype(F32)
    acc[pl.ds(0, TOP), CC:] += last[:, CC:]

    @pl.when(sp == 0)
    def _():
        proj[pl.ds(0, EDGE), :] = jnp.zeros((EDGE, CC), F32)

    def edge_down():
        return pltpu.make_async_remote_copy(
            src_ref=proj.at[pl.ds(EDGE, 8), :],
            dst_ref=proj.at[pl.ds(EDGE + TOK, 8), :],
            send_sem=hsend.at[1],
            recv_sem=hrecv.at[1],
            device_id={"sp": lax.rem(sp + NSP - 1, NSP)},
            device_id_type=MESH,
        )

    @pl.when(sp > 0)
    def _():
        edge_down().start()

    bias = jnp.concatenate([biasb[0:1, :], biasb[1:2, :]], axis=1)
    rate = jnp.concatenate([rateb[0:1, :], rateb[1:2, :]], axis=1)
    row = iota((SPAN, SPAN), 0)
    col = iota((SPAN, SPAN), 1)
    later = jnp.where(col > row, 1.0, 0.0)
    earlier = jnp.where(col < row, 1.0, 0.0)

    def weights_of(k):
        dt_raw = acc[pl.ds(EDGE + k * SPAN, SPAN), CC:].astype(BF16).astype(F32)
        v = dt_raw + bias
        step = jnp.maximum(v, 0.0) + jnp.log1p(jnp.exp(-jnp.abs(v)))
        a = -(step * rate) / LEN
        tail = jnp.dot(later, a, precision=lax.Precision.HIGHEST, preferred_element_type=F32)
        head = jnp.dot(earlier, a, precision=lax.Precision.HIGHEST, preferred_element_type=F32)
        w = jnp.exp(jnp.where(col < H, tail, head)) * step
        redy[y, k : k + 1, pl.ds(512, 128)] = jnp.sum(a, axis=0, keepdims=True)
        high = w.astype(BF16)
        low = (w - high.astype(F32)).astype(BF16)
        return jnp.concatenate([high, low], axis=1)

    taps = [cxb[...].astype(F32), cbb[...].astype(F32)]

    def convolve(start, count):
        for block in range(CC // 256):
            tap = taps[0][:, block * 256 : (block + 1) * 256] if block < 2 else taps[1]
            cols = pl.ds(block * 256, 256)
            total = jnp.zeros((count, 256), F32)
            for o in range(KW):
                total = total + tap[o : o + 1] * proj[pl.ds(start + EDGE - 2 + o, count), cols]
            mixed[pl.ds(start, count), cols] = jax.nn.silu(total).astype(BF16)

    order = (4 * (row % 32) + row // 32 == col)
    order_t = jnp.where(order, 1.0, 0.0).astype(BF16)
    contract_last = (((1,), (1,)), ((), ()))
    queries = []
    for g in range(2):
        q8 = jnp.broadcast_to(qb[0, g : g + 1, :].astype(F32), (8, N)).astype(BF16)
        queries.append(
            lax.dot_general(q8, order_t, contract_last, preferred_element_type=F32).astype(BF16)
        )
    half = iota((32, 128), 1) < P_SIZE
    chosen = rb[0]

    def state_copy(k, d, s):
        return pltpu.make_async_remote_copy(
            src_ref=sendb.at[d, k],
            dst_ref=cache.at[2 * s + k],
            send_sem=asend,
            recv_sem=arecv,
            device_id={"sp": d},
            device_id_type=MESH,
        )

    across_y = [lax.rem(y + dy, NY) for dy in range(NY)]
    across_z = [lax.rem(z + dz, NZ) * NY for dz in range(NZ)]
    distances = (4, 5, 3, 6, 2, 7, 1)

    def send_states(k, first, last):
        for dy in distances[first:last]:
            for dz in range(NZ):
                state_copy(k, across_z[dz] + across_y[dy], sp).start()

    def send_column(k):
        for dz in range(1, NZ):
            state_copy(k, across_z[dz] + y, sp).start()

    own_out = []

    def states_of(k, pair):
        rows = pl.ds(k * SPAN, SPAN)
        keys_t = [
            lax.dot_general(
                order_t, mixed[rows, pl.ds(XC + g * N, N)], contract_last,
                preferred_element_type=F32,
            ).astype(BF16)
            for g in range(2)
        ]
        for e in range(2):
            wide = jnp.dot(pair, expand[:, pl.ds(e * 512, 512)], preferred_element_type=F32)
            weighted = (mixed[rows, pl.ds(0, XC)].astype(F32) * wide).astype(BF16)
            for g in range(2):
                state = jnp.dot(
                    keys_t[g], weighted[:, g * 256 : (g + 1) * 256], preferred_element_type=F32
                )
                held[e, g] = state
    def read_of(k):
        for e in range(2):
            for g in range(2):
                read = jnp.dot(
                    queries[g], held[e, g].astype(BF16), preferred_element_type=F32
                )
                ybuf[e : e + 1, pl.ds(g * 256, 256)] = read[0:1]
        at = jnp.full((1, 512), 2 * sp + k, jnp.int32)
        pick = jnp.full((1, 512), chosen, jnp.int32)
        redy[y, k : k + 1, pl.ds(0, 512)] = jnp.where(at <= pick, ybuf[0:1, :], 0.0) + jnp.where(
            at >= pick, ybuf[1:2, :], 0.0
        )

    def arrange(k):
        for e in range(2):
            for g in range(2):
                for j in range(2):
                    for a in range(2):
                        lanes = pl.ds(128 * j, 128)
                        one = held[e, g, pl.ds(64 * a, 32), lanes]
                        two = held[e, g, pl.ds(64 * a + 32, 32), lanes]
                        first = jnp.where(half, one, pltpu.roll(two, 64, 1))
                        second = jnp.where(half, pltpu.roll(one, 64, 1), two)
                        h = 4 * g + 2 * j
                        sbuf[a, pl.ds(h, 32, stride=8), :] = first
                        sbuf[a, pl.ds(h + 1, 32, stride=8), :] = second
            for a in range(2):
                sendb[:, k, e, :, pl.ds(a * 128, 128)] = (
                    sbuf[a].reshape(NSP, 8, 128).astype(BF16)
                )
        c = pltpu.make_async_copy(sendb.at[sp, k], cache.at[2 * sp + k], own_sem.at[k])
        c.start()
        own_out.append(c)

    pair = weights_of(0)
    for first in range(0, SPAN, 16):
        convolve(first, 16)
    pass_on(2)
    pl.semaphore_wait(stage.at[2], 2)
    states_of(0, pair)
    arrange(0)
    send_column(0)
    send_states(0, 0, EARLY)
    read_of(0)

    for slot in (partner, *ring, twin(right), twin(left)):
        if slot is not right and slot is not left and slot is not across:
            arrive(slot, 2)
        add(slot, TOP, ROWS_B)
    arrive(twin(across), 2)
    last = product(twin(across), TOP, ROWS_B)
    rest = pl.ds(TOP, ROWS_B)
    proj[rest, :] = (acc[rest, :CC] + last[:, :CC]).astype(BF16).astype(F32)
    acc[rest, CC:] += last[:, CC:]
    pair = weights_of(1)
    for first in range(SPAN, TOK - 16, 16):
        convolve(first, 16)

    @pl.when(sp < NSP - 1)
    def _():
        edge_down().wait_recv()

    @pl.when(sp == NSP - 1)
    def _():
        proj[pl.ds(EDGE + TOK, 8), :] = jnp.zeros((8, CC), F32)

    convolve(TOK - 16, 16)
    states_of(1, pair)
    read_of(1)

    def exchange(buffer, me, count, sems, place):
        for i in range(1, count):
            other = lax.rem(me + i, count)
            pltpu.make_async_remote_copy(
                src_ref=buffer.at[me],
                dst_ref=buffer.at[me],
                send_sem=sems.at[0],
                recv_sem=sems.at[1],
                device_id=place(other),
                device_id_type=MESH,
            ).start()

        return pltpu.make_async_remote_copy(
            src_ref=buffer.at[pl.ds(0, count - 1)],
            dst_ref=buffer.at[pl.ds(0, count - 1)],
            send_sem=sems.at[0],
            recv_sem=sems.at[1],
            device_id=place(me),
            device_id_type=MESH,
        )

    y_all = exchange(redy, y, NY, ysems, lambda d: {"sp": z * NY + d})
    send_states(0, EARLY, 7)
    arrange(1)
    send_column(1)
    send_states(1, 0, MID)

    def spread(rows):
        high = rows.astype(BF16)
        low = (rows - high.astype(F32)).astype(BF16)
        return jnp.dot(
            jnp.concatenate([high, low], axis=1),
            expand[:, pl.ds(0, 512)],
            preferred_element_type=F32,
        )

    gate = jax.nn.silu(gateb[0].astype(F32))
    y_all.wait_recv()
    base = 2 * NY * z
    ahead_lane = iota((8, 128), 1) < H
    block_log = jnp.zeros((8, 128), F32)
    span_logs = [jnp.zeros((8, 128), F32), jnp.zeros((8, 128), F32)]
    pick = jnp.full((8, 128), chosen, jnp.int32)
    span_at = [base + 2 * iota((8, 128), 0) + k for k in range(2)]
    for other in range(2 * NY):
        log = jnp.broadcast_to(
            redy[other // 2, other % 2 : other % 2 + 1, pl.ds(512, 128)], (8, 128)
        )
        here = jnp.full((8, 128), base + other, jnp.int32)
        log = jnp.where(ahead_lane, jnp.where(here <= pick, log, 0.0), jnp.where(here >= pick, log, 0.0))
        block_log = block_log + log
        for k in range(2):
            counted = jnp.where(
                ahead_lane,
                jnp.where(here > span_at[k], log, 0.0),
                jnp.where(here < span_at[k], log, 0.0),
            )
            span_logs[k] = span_logs[k] + counted
    span_weights = [jnp.exp(t + pltpu.roll(t, H, 1)) for t in span_logs]
    wide_weight = spread(jnp.concatenate(span_weights, axis=0))
    partial = jnp.zeros((8, 512), F32)
    for k in range(2):
        partial = partial + wide_weight[8 * k : 8 * k + 8] * redy[:, k, pl.ds(0, 512)]
    redz[z, :, pl.ds(0, 512)] = jnp.sum(partial, axis=0, keepdims=True)
    redz[z, :, pl.ds(512, 128)] = block_log[0:1]
    z_all = exchange(redz, z, NZ, zsems, lambda d: {"sp": d * NY + y})
    send_states(1, MID, 7)
    z_all.wait_recv()
    lane = iota((1, 128), 1)
    block_rows = []
    for block in range(NZ):
        after = jnp.zeros((1, 128), F32)
        before = jnp.zeros((1, 128), F32)
        for other in range(block + 1, NZ):
            after = after + redz[other, :, pl.ds(512, 128)]
        for other in range(block):
            before = before + redz[other, :, pl.ds(512, 128)]
        block_rows.append(jnp.where(lane < H, after, before))
    block_rows = block_rows + [jnp.zeros((8 - NZ, 128), F32)]
    logs = jnp.concatenate(block_rows, axis=0)
    block_factor = spread(jnp.exp(logs + pltpu.roll(logs, H, 1)))
    total = jnp.zeros((1, 512), F32)
    for block in range(NZ):
        total = total + block_factor[block : block + 1] * redz[block, :, pl.ds(0, 512)]
    for h in range(8):
        tot8[h : h + 1, :] = total[:, h * P_SIZE : (h + 1) * P_SIZE]
    gated = tot8[...] * gate
    squares = jnp.sum(jnp.sum(gated * gated, axis=0, keepdims=True), axis=1, keepdims=True)
    reds[tp] = jnp.broadcast_to(squares, (1, 128))
    s_all = exchange(reds, tp, NTP, ssems, lambda d: {"tp": d})
    s_all.wait_recv()
    square_sum = jnp.sum(reds[...], axis=0)[:, :64]
    scale = lax.rsqrt(square_sum / (H * P_SIZE) + EPSILON)
    first_read[0] = (gated * scale * gainb[...]).astype(BF16)

    for j, (start, count) in enumerate(pieces):
        sent = slab.at[pl.ds(0, NTP - 1), pl.ds(start, count), :]
        pltpu.make_async_remote_copy(
            src_ref=sent,
            dst_ref=sent,
            send_sem=gsend.at[j],
            recv_sem=gsend.at[j],
            device_id={"tp": partner},
            device_id_type=MESH,
        ).wait_send()

    @pl.when(sp < NSP - 1)
    def _():
        edge_in().wait_send()

    @pl.when(sp > 0)
    def _():
        edge_down().wait_send()

    y_all.wait_send()
    z_all.wait_send()
    s_all.wait_send()
    every = cache.at[pl.ds(0, 2 * NSP - 2)]
    states = pltpu.make_async_remote_copy(
        src_ref=every,
        dst_ref=every,
        send_sem=asend,
        recv_sem=arecv,
        device_id={"sp": sp},
        device_id_type=MESH,
    )
    states.wait_recv()
    states.wait_send()
    for c in own_out:
        c.wait()


def write_out(cache, first_read, cache_out, first_out, sems):
    copies = [
        pltpu.make_async_copy(
            cache.at[pl.ds(16 * i, 16)], cache_out.at[pl.ds(16 * i, 16)], sems.at[i]
        )
        for i in range(4)
    ]
    copies.append(pltpu.make_async_copy(first_read, first_out, sems.at[4]))
    for c in copies:
        c.start()
    for c in copies:
        c.wait()


def per_device(*args):
    dma = pltpu.SemaphoreType.DMA
    any_spec = pl.BlockSpec(memory_space=pl.ANY)
    vmem_spec = pl.BlockSpec(memory_space=pltpu.VMEM)
    shapes = (
        jax.ShapeDtypeStruct((64, 2, 8, 256), BF16),
        jax.ShapeDtypeStruct((1, 8, 64), BF16),
    )
    results = pl.pallas_call(
        kernel,
        out_shape=tuple(pltpu.VMEM(t.shape, t.dtype) for t in shapes),
        in_specs=[any_spec] * 12,
        out_specs=(vmem_spec, vmem_spec),
        scratch_shapes=[
            pltpu.VMEM((NTP, EDGE + TOK, FEAT), BF16),
            pltpu.VMEM((2048, WC), BF16),
            pltpu.VMEM((EDGE + TOK, WC), F32),
            pltpu.VMEM((EDGE + TOK + 8, CC), F32),
            pltpu.VMEM((TOK, CC), BF16),
            pltpu.VMEM((2, 2, N, 256), F32),
            pltpu.VMEM((2, H), F32),
            pltpu.VMEM((2, H), F32),
            pltpu.VMEM((KW, XC), BF16),
            pltpu.VMEM((KW, BC), BF16),
            pltpu.VMEM((1, 2, N), BF16),
            pltpu.VMEM((1, 8, P_SIZE), BF16),
            pltpu.VMEM((8, P_SIZE), F32),
            pltpu.SMEM((1,), jnp.int32),
            pltpu.VMEM((256, 1024), BF16),
            pltpu.VMEM((2, 256, 128), F32),
            pltpu.VMEM((NSP, 2, 2, 8, 256), BF16),
            pltpu.VMEM((8, 512), F32),
            pltpu.VMEM((NY, 2, 640), F32),
            pltpu.VMEM((NZ, 1, 640), F32),
            pltpu.VMEM((NTP, 1, 128), F32),
            pltpu.VMEM((8, P_SIZE), F32),
            dma,
            dma((15,)),
            dma((3,)),
            dma((NTP, 3)),
            dma((2,)),
            dma((2,)),
            dma,
            dma,
            dma((2,)),
            dma((2,)),
            dma((2,)),
            dma((2,)),
            pltpu.SemaphoreType.REGULAR((3,)),
        ],
        compiler_params=pltpu.CompilerParams(collective_id=0, has_side_effects=True),
    )(*args)
    results = [pltpu.with_memory_space_constraint(r, pltpu.VMEM) for r in results]
    return pl.pallas_call(
        write_out,
        out_shape=shapes,
        in_specs=[vmem_spec] * 2,
        out_specs=(any_spec, any_spec),
        scratch_shapes=[dma((5,))],
    )(*results)


def solution(mesh):
    return jax.shard_map(
        per_device,
        mesh=mesh,
        in_specs=(
            P(("gr", "sp"), "tp"),
            P(None, "tp"),
            P(None, "tp"),
            P(),
            P(),
            P(),
            P(None, "tp"),
            P(None, "tp"),
            P("gr", "tp", None),
            P("gr", "tp", None),
            P("gr"),
            P("tp", None),
        ),
        out_specs=(P("gr", None, "tp", "sp"), P("gr", "tp", None)),
        check_vma=False,
    )
```

```python
import jax
import jax.numpy as jnp
from jax import lax
from jax.experimental import pallas as pl
from jax.experimental.pallas import tpu as pltpu
from jax.sharding import PartitionSpec as P

H = 64
P_SIZE = 64
G = 16
N = 128
KW = 5
SPAN = 128
EPSILON = 1e-06
LEN = 8192
NY = 8
NZ = 4
NX = 4
NSP = 32
NTP = 8
TOK = 256
FEAT = 256
XC = 512
BC = 256
CC = 768
WC = 896
EDGE = 16
ROWS_A = 144
ROWS_B = TOK - ROWS_A
TOP = EDGE + ROWS_A
EARLY = 2
MID = 0

MESH = pl.DeviceIdType.MESH
F32 = jnp.float32
BF16 = jnp.bfloat16


def iota(shape, dim):
    return lax.broadcasted_iota(jnp.int32, shape, dim)


def kernel(
    inputs, x_weight, b_weight, dt_weight, dt_bias, decay_rate, conv_x, conv_b,
    query_c, query_gate, read_span, read_gain,
    cache, first_read,
    slab, wbuf, acc, proj, mixed, held, biasb, rateb, cxb, cbb, qb, gateb, gainb, rb,
    expand, sbuf, sendb, ybuf, redy, redz, reds, tot8,
    in_sem, load_sems, gsend, grecv, hsend, hrecv, asend, arecv,
    ysems, zsems, ssems, own_sem, stage,
):
    sp = lax.axis_index("sp")
    tp = lax.axis_index("tp")
    y = lax.rem(sp, NY)
    z = lax.div(sp, NY)
    core = lax.rem(tp, 2)
    partner = tp + 1 - 2 * core
    right = lax.rem(tp + 2, NTP)
    left = lax.rem(tp + NTP - 2, NTP)
    across = lax.rem(tp + NTP // 2, NTP)

    own_in = pltpu.make_async_copy(inputs, slab.at[tp, pl.ds(EDGE, TOK), :], in_sem)
    own_in.start()
    loads = []
    for width, weight, first, cuts in (
        (XC, x_weight, 0, 4), (BC, b_weight, XC, 2), (128, dt_weight, CC, 1)
    ):
        for i in range(cuts):
            depth = pl.ds(i * (2048 // cuts), 2048 // cuts)
            loads.append((weight.at[depth, :], wbuf.at[depth, pl.ds(first, width)]))
    loads += [
        (dt_bias, biasb),
        (decay_rate, rateb),
        (conv_x, cxb),
        (conv_b, cbb),
        (query_c, qb),
        (query_gate, gateb),
        (read_gain, gainb),
        (read_span, rb),
    ]
    copies = []
    for i, (src, dst) in enumerate(loads):
        c = pltpu.make_async_copy(src, dst, load_sems.at[i])
        c.start(priority=1)
        copies.append(c)

    barrier = pltpu.get_barrier_semaphore()

    def at_y(other):
        return {"sp": z * NY + lax.rem(other, NY)}

    for i in range(1, NTP):
        pl.semaphore_signal(
            barrier, inc=1, device_id={"tp": lax.rem(tp + i, NTP)}, device_id_type=MESH
        )
    for i in range(1, NZ):
        pl.semaphore_signal(
            barrier, inc=1, device_id={"sp": lax.rem(z + i, NZ) * NY + y}, device_id_type=MESH
        )
    for side in (1, NY - 1):
        pl.semaphore_signal(barrier, inc=1, device_id=at_y(y + side), device_id_type=MESH)
    for side in (1, NSP - 1):
        pl.semaphore_signal(
            barrier, inc=1, device_id={"sp": lax.rem(sp + side, NSP)}, device_id_type=MESH
        )

    def tell(index, distance):
        for side in (distance, NY - distance):
            pl.semaphore_signal(
                stage.at[index], inc=1, device_id=at_y(y + side), device_id_type=MESH
            )

    @pl.when(sp == 0)
    def _():
        slab[tp, pl.ds(0, EDGE), :] = jnp.zeros((EDGE, FEAT), BF16)

    own_in.wait()
    pl.semaphore_wait(barrier, NTP - 1 + NZ - 1 + 4)
    tell(0, 1)

    def edge_in():
        return pltpu.make_async_remote_copy(
            src_ref=slab.at[tp, pl.ds(TOK, EDGE), :],
            dst_ref=slab.at[tp, pl.ds(0, EDGE), :],
            send_sem=hsend.at[0],
            recv_sem=hrecv.at[0],
            device_id={"sp": lax.rem(sp + 1, NSP)},
            device_id_type=MESH,
        )

    @pl.when(sp < NSP - 1)
    def _():
        edge_in().start()

    pieces = [(EDGE, ROWS_A), (0, EDGE), (TOP, ROWS_B)]

    def part(slot, j):
        return slab.at[slot, pl.ds(*pieces[j]), :]

    def forward(slot, j, dest):
        c = pltpu.make_async_remote_copy(
            src_ref=part(slot, j),
            dst_ref=part(slot, j),
            send_sem=gsend.at[j],
            recv_sem=grecv.at[slot, j],
            device_id={"tp": dest},
            device_id_type=MESH,
        )
        c.start()

    def arrive(slot, j):
        pltpu.make_async_remote_copy(
            src_ref=part(slot, j),
            dst_ref=part(slot, j),
            send_sem=gsend.at[j],
            recv_sem=grecv.at[slot, j],
            device_id={"tp": partner},
            device_id_type=MESH,
        ).wait_recv()

    def send_own(j):
        for dest in (across, right, left, partner):
            forward(tp, j, dest)

    ring = (right, left, across)

    def pass_on(j):
        for slot in (across, right, left):
            arrive(slot, j)
            forward(slot, j, partner)

    def twin(slot):
        return slot + 1 - 2 * core

    def product(slot, start, count):
        rows = pl.ds(pl.multiple_of(slot * FEAT, FEAT), FEAT)
        return jnp.dot(
            slab[slot, pl.ds(start, count), :], wbuf[rows, :], preferred_element_type=F32
        )

    def add(slot, start, count):
        acc[pl.ds(start, count), :] += product(slot, start, count)

    send_own(0)
    er = iota((256, 1024), 0) % 128
    ec = iota((256, 1024), 1)
    expand[...] = jnp.where(
        er == (ec // 512) * H + tp * 8 + (ec % 512) // P_SIZE, 1.0, 0.0
    ).astype(BF16)

    @pl.when(sp > 0)
    def _():
        edge_in().wait_recv()

    send_own(1)
    send_own(2)
    for c in copies:
        c.wait()
    acc[pl.ds(0, TOP), :] = product(tp, 0, TOP)
    pass_on(0)
    pl.semaphore_wait(stage.at[0], 2)
    tell(1, 2)
    acc[pl.ds(TOP, ROWS_B), :] = product(tp, TOP, ROWS_B)
    for j in (0, 1):
        arrive(partner, j)
    add(partner, 0, TOP)
    pass_on(1)
    for slot in ring:
        add(slot, 0, TOP)
    for slot in ring[:2]:
        for j in (0, 1):
            arrive(twin(slot), j)
        add(twin(slot), 0, TOP)
    pl.semaphore_wait(stage.at[1], 2)
    tell(2, 1)
    for j in (0, 1):
        arrive(twin(across), j)
    last = product(twin(across), 0, TOP)
    proj[pl.ds(0, TOP), :] = (acc[pl.ds(0, TOP), :CC] + last[:, :CC]).astype(BF16).astype(F32)
    acc[pl.ds(0, TOP), CC:] += last[:, CC:]

    @pl.when(sp == 0)
    def _():
        proj[pl.ds(0, EDGE), :] = jnp.zeros((EDGE, CC), F32)

    def edge_down():
        return pltpu.make_async_remote_copy(
            src_ref=proj.at[pl.ds(EDGE, 8), :],
            dst_ref=proj.at[pl.ds(EDGE + TOK, 8), :],
            send_sem=hsend.at[1],
            recv_sem=hrecv.at[1],
            device_id={"sp": lax.rem(sp + NSP - 1, NSP)},
            device_id_type=MESH,
        )

    @pl.when(sp > 0)
    def _():
        edge_down().start()

    bias = jnp.concatenate([biasb[0:1, :], biasb[1:2, :]], axis=1)
    rate = jnp.concatenate([rateb[0:1, :], rateb[1:2, :]], axis=1)
    row = iota((SPAN, SPAN), 0)
    col = iota((SPAN, SPAN), 1)
    later = jnp.where(col > row, 1.0, 0.0)
    earlier = jnp.where(col < row, 1.0, 0.0)

    def weights_of(k):
        dt_raw = acc[pl.ds(EDGE + k * SPAN, SPAN), CC:].astype(BF16).astype(F32)
        v = dt_raw + bias
        step = jnp.maximum(v, 0.0) + jnp.log1p(jnp.exp(-jnp.abs(v)))
        a = -(step * rate) / LEN
        tail = jnp.dot(later, a, precision=lax.Precision.HIGHEST, preferred_element_type=F32)
        head = jnp.dot(earlier, a, precision=lax.Precision.HIGHEST, preferred_element_type=F32)
        w = jnp.exp(jnp.where(col < H, tail, head)) * step
        redy[y, k : k + 1, pl.ds(512, 128)] = jnp.sum(a, axis=0, keepdims=True)
        high = w.astype(BF16)
        low = (w - high.astype(F32)).astype(BF16)
        return jnp.concatenate([high, low], axis=1)

    taps = [cxb[...].astype(F32), cbb[...].astype(F32)]

    def convolve(start, count):
        for block in range(CC // 256):
            tap = taps[0][:, block * 256 : (block + 1) * 256] if block < 2 else taps[1]
            cols = pl.ds(block * 256, 256)
            total = jnp.zeros((count, 256), F32)
            for o in range(KW):
                total = total + tap[o : o + 1] * proj[pl.ds(start + EDGE - 2 + o, count), cols]
            mixed[pl.ds(start, count), cols] = jax.nn.silu(total).astype(BF16)

    order = (4 * (row % 32) + row // 32 == col)
    order_t = jnp.where(order, 1.0, 0.0).astype(BF16)
    contract_last = (((1,), (1,)), ((), ()))
    queries = []
    for g in range(2):
        q8 = jnp.broadcast_to(qb[0, g : g + 1, :].astype(F32), (8, N)).astype(BF16)
        queries.append(
            lax.dot_general(q8, order_t, contract_last, preferred_element_type=F32).astype(BF16)
        )
    half = iota((32, 128), 1) < P_SIZE
    chosen = rb[0]

    def state_copy(k, d, s):
        return pltpu.make_async_remote_copy(
            src_ref=sendb.at[d, k],
            dst_ref=cache.at[2 * s + k],
            send_sem=asend,
            recv_sem=arecv,
            device_id={"sp": d},
            device_id_type=MESH,
        )

    across_y = [lax.rem(y + dy, NY) for dy in range(NY)]
    across_z = [lax.rem(z + dz, NZ) * NY for dz in range(NZ)]
    distances = (4, 5, 3, 6, 2, 7, 1)

    def send_states(k, first, last):
        for dy in distances[first:last]:
            for dz in range(NZ):
                state_copy(k, across_z[dz] + across_y[dy], sp).start()

    def send_column(k):
        for dz in range(1, NZ):
            state_copy(k, across_z[dz] + y, sp).start()

    own_out = []

    def states_of(k, pair):
        rows = pl.ds(k * SPAN, SPAN)
        keys_t = [
            lax.dot_general(
                order_t, mixed[rows, pl.ds(XC + g * N, N)], contract_last,
                preferred_element_type=F32,
            ).astype(BF16)
            for g in range(2)
        ]
        for e in range(2):
            wide = jnp.dot(pair, expand[:, pl.ds(e * 512, 512)], preferred_element_type=F32)
            weighted = (mixed[rows, pl.ds(0, XC)].astype(F32) * wide).astype(BF16)
            for g in range(2):
                state = jnp.dot(
                    keys_t[g], weighted[:, g * 256 : (g + 1) * 256], preferred_element_type=F32
                )
                read = jnp.dot(queries[g], state.astype(BF16), preferred_element_type=F32)
                ybuf[e : e + 1, pl.ds(g * 256, 256)] = read[0:1]
                held[e, g] = state
        at = jnp.full((1, 512), 2 * sp + k, jnp.int32)
        pick = jnp.full((1, 512), chosen, jnp.int32)
        redy[y, k : k + 1, pl.ds(0, 512)] = jnp.where(at <= pick, ybuf[0:1, :], 0.0) + jnp.where(
            at >= pick, ybuf[1:2, :], 0.0
        )

    def arrange(k):
        for e in range(2):
            for g in range(2):
                for j in range(2):
                    for a in range(2):
                        lanes = pl.ds(128 * j, 128)
                        one = held[e, g, pl.ds(64 * a, 32), lanes]
                        two = held[e, g, pl.ds(64 * a + 32, 32), lanes]
                        first = jnp.where(half, one, pltpu.roll(two, 64, 1))
                        second = jnp.where(half, pltpu.roll(one, 64, 1), two)
                        h = 4 * g + 2 * j
                        sbuf[a, pl.ds(h, 32, stride=8), :] = first
                        sbuf[a, pl.ds(h + 1, 32, stride=8), :] = second
            for a in range(2):
                sendb[:, k, e, :, pl.ds(a * 128, 128)] = (
                    sbuf[a].reshape(NSP, 8, 128).astype(BF16)
                )
        c = pltpu.make_async_copy(sendb.at[sp, k], cache.at[2 * sp + k], own_sem.at[k])
        c.start()
        own_out.append(c)

    pair = weights_of(0)
    for first in range(0, SPAN, 16):
        convolve(first, 16)
    pass_on(2)
    pl.semaphore_wait(stage.at[2], 2)
    states_of(0, pair)
    arrange(0)
    send_column(0)
    send_states(0, 0, EARLY)

    for slot in (partner, *ring, twin(right), twin(left)):
        if slot is not right and slot is not left and slot is not across:
            arrive(slot, 2)
        add(slot, TOP, ROWS_B)
    arrive(twin(across), 2)
    last = product(twin(across), TOP, ROWS_B)
    rest = pl.ds(TOP, ROWS_B)
    proj[rest, :] = (acc[rest, :CC] + last[:, :CC]).astype(BF16).astype(F32)
    acc[rest, CC:] += last[:, CC:]
    pair = weights_of(1)
    for first in range(SPAN, TOK - 16, 16):
        convolve(first, 16)

    @pl.when(sp < NSP - 1)
    def _():
        edge_down().wait_recv()

    @pl.when(sp == NSP - 1)
    def _():
        proj[pl.ds(EDGE + TOK, 8), :] = jnp.zeros((8, CC), F32)

    convolve(TOK - 16, 16)
    states_of(1, pair)

    def exchange(buffer, me, count, sems, place):
        for i in range(1, count):
            other = lax.rem(me + i, count)
            pltpu.make_async_remote_copy(
                src_ref=buffer.at[me],
                dst_ref=buffer.at[me],
                send_sem=sems.at[0],
                recv_sem=sems.at[1],
                device_id=place(other),
                device_id_type=MESH,
            ).start()

        return pltpu.make_async_remote_copy(
            src_ref=buffer.at[pl.ds(0, count - 1)],
            dst_ref=buffer.at[pl.ds(0, count - 1)],
            send_sem=sems.at[0],
            recv_sem=sems.at[1],
            device_id=place(me),
            device_id_type=MESH,
        )

    y_all = exchange(redy, y, NY, ysems, lambda d: {"sp": z * NY + d})
    send_states(0, EARLY, 7)
    arrange(1)
    send_column(1)
    send_states(1, 0, MID)

    def spread(rows):
        high = rows.astype(BF16)
        low = (rows - high.astype(F32)).astype(BF16)
        return jnp.dot(
            jnp.concatenate([high, low], axis=1),
            expand[:, pl.ds(0, 512)],
            preferred_element_type=F32,
        )

    gate = jax.nn.silu(gateb[0].astype(F32))
    y_all.wait_recv()
    base = 2 * NY * z
    ahead_lane = iota((8, 128), 1) < H
    block_log = jnp.zeros((8, 128), F32)
    span_logs = [jnp.zeros((8, 128), F32), jnp.zeros((8, 128), F32)]
    pick = jnp.full((8, 128), chosen, jnp.int32)
    span_at = [base + 2 * iota((8, 128), 0) + k for k in range(2)]
    for other in range(2 * NY):
        log = jnp.broadcast_to(
            redy[other // 2, other % 2 : other % 2 + 1, pl.ds(512, 128)], (8, 128)
        )
        here = jnp.full((8, 128), base + other, jnp.int32)
        log = jnp.where(ahead_lane, jnp.where(here <= pick, log, 0.0), jnp.where(here >= pick, log, 0.0))
        block_log = block_log + log
        for k in range(2):
            counted = jnp.where(
                ahead_lane,
                jnp.where(here > span_at[k], log, 0.0),
                jnp.where(here < span_at[k], log, 0.0),
            )
            span_logs[k] = span_logs[k] + counted
    span_weights = [jnp.exp(t + pltpu.roll(t, H, 1)) for t in span_logs]
    wide_weight = spread(jnp.concatenate(span_weights, axis=0))
    partial = jnp.zeros((8, 512), F32)
    for k in range(2):
        partial = partial + wide_weight[8 * k : 8 * k + 8] * redy[:, k, pl.ds(0, 512)]
    redz[z, :, pl.ds(0, 512)] = jnp.sum(partial, axis=0, keepdims=True)
    redz[z, :, pl.ds(512, 128)] = block_log[0:1]
    z_all = exchange(redz, z, NZ, zsems, lambda d: {"sp": d * NY + y})
    send_states(1, MID, 7)
    z_all.wait_recv()
    lane = iota((1, 128), 1)
    block_rows = []
    for block in range(NZ):
        after = jnp.zeros((1, 128), F32)
        before = jnp.zeros((1, 128), F32)
        for other in range(block + 1, NZ):
            after = after + redz[other, :, pl.ds(512, 128)]
        for other in range(block):
            before = before + redz[other, :, pl.ds(512, 128)]
        block_rows.append(jnp.where(lane < H, after, before))
    block_rows = block_rows + [jnp.zeros((8 - NZ, 128), F32)]
    logs = jnp.concatenate(block_rows, axis=0)
    block_factor = spread(jnp.exp(logs + pltpu.roll(logs, H, 1)))
    total = jnp.zeros((1, 512), F32)
    for block in range(NZ):
        total = total + block_factor[block : block + 1] * redz[block, :, pl.ds(0, 512)]
    for h in range(8):
        tot8[h : h + 1, :] = total[:, h * P_SIZE : (h + 1) * P_SIZE]
    gated = tot8[...] * gate
    squares = jnp.sum(jnp.sum(gated * gated, axis=0, keepdims=True), axis=1, keepdims=True)
    reds[tp] = jnp.broadcast_to(squares, (1, 128))
    s_all = exchange(reds, tp, NTP, ssems, lambda d: {"tp": d})
    s_all.wait_recv()
    square_sum = jnp.sum(reds[...], axis=0)[:, :64]
    scale = lax.rsqrt(square_sum / (H * P_SIZE) + EPSILON)
    first_read[0] = (gated * scale * gainb[...]).astype(BF16)

    for j, (start, count) in enumerate(pieces):
        sent = slab.at[pl.ds(0, NTP - 1), pl.ds(start, count), :]
        pltpu.make_async_remote_copy(
            src_ref=sent,
            dst_ref=sent,
            send_sem=gsend.at[j],
            recv_sem=gsend.at[j],
            device_id={"tp": partner},
            device_id_type=MESH,
        ).wait_send()

    @pl.when(sp < NSP - 1)
    def _():
        edge_in().wait_send()

    @pl.when(sp > 0)
    def _():
        edge_down().wait_send()

    y_all.wait_send()
    z_all.wait_send()
    s_all.wait_send()
    every = cache.at[pl.ds(0, 2 * NSP - 2)]
    states = pltpu.make_async_remote_copy(
        src_ref=every,
        dst_ref=every,
        send_sem=asend,
        recv_sem=arecv,
        device_id={"sp": sp},
        device_id_type=MESH,
    )
    states.wait_recv()
    states.wait_send()
    for c in own_out:
        c.wait()


def write_out(cache, first_read, cache_out, first_out, sems):
    copies = [
        pltpu.make_async_copy(
            cache.at[pl.ds(16 * i, 16)], cache_out.at[pl.ds(16 * i, 16)], sems.at[i]
        )
        for i in range(4)
    ]
    copies.append(pltpu.make_async_copy(first_read, first_out, sems.at[4]))
    for c in copies:
        c.start()
    for c in copies:
        c.wait()


def per_device(*args):
    dma = pltpu.SemaphoreType.DMA
    any_spec = pl.BlockSpec(memory_space=pl.ANY)
    vmem_spec = pl.BlockSpec(memory_space=pltpu.VMEM)
    shapes = (
        jax.ShapeDtypeStruct((64, 2, 8, 256), BF16),
        jax.ShapeDtypeStruct((1, 8, 64), BF16),
    )
    results = pl.pallas_call(
        kernel,
        out_shape=tuple(pltpu.VMEM(t.shape, t.dtype) for t in shapes),
        in_specs=[any_spec] * 12,
        out_specs=(vmem_spec, vmem_spec),
        scratch_shapes=[
            pltpu.VMEM((NTP, EDGE + TOK, FEAT), BF16),
            pltpu.VMEM((2048, WC), BF16),
            pltpu.VMEM((EDGE + TOK, WC), F32),
            pltpu.VMEM((EDGE + TOK + 8, CC), F32),
            pltpu.VMEM((TOK, CC), BF16),
            pltpu.VMEM((2, 2, N, 256), F32),
            pltpu.VMEM((2, H), F32),
            pltpu.VMEM((2, H), F32),
            pltpu.VMEM((KW, XC), BF16),
            pltpu.VMEM((KW, BC), BF16),
            pltpu.VMEM((1, 2, N), BF16),
            pltpu.VMEM((1, 8, P_SIZE), BF16),
            pltpu.VMEM((8, P_SIZE), F32),
            pltpu.SMEM((1,), jnp.int32),
            pltpu.VMEM((256, 1024), BF16),
            pltpu.VMEM((2, 256, 128), F32),
            pltpu.VMEM((NSP, 2, 2, 8, 256), BF16),
            pltpu.VMEM((8, 512), F32),
            pltpu.VMEM((NY, 2, 640), F32),
            pltpu.VMEM((NZ, 1, 640), F32),
            pltpu.VMEM((NTP, 1, 128), F32),
            pltpu.VMEM((8, P_SIZE), F32),
            dma,
            dma((15,)),
            dma((3,)),
            dma((NTP, 3)),
            dma((2,)),
            dma((2,)),
            dma,
            dma,
            dma((2,)),
            dma((2,)),
            dma((2,)),
            dma((2,)),
            pltpu.SemaphoreType.REGULAR((3,)),
        ],
        compiler_params=pltpu.CompilerParams(collective_id=0, has_side_effects=True),
    )(*args)
    results = [pltpu.with_memory_space_constraint(r, pltpu.VMEM) for r in results]
    return pl.pallas_call(
        write_out,
        out_shape=shapes,
        in_specs=[vmem_spec] * 2,
        out_specs=(any_spec, any_spec),
        scratch_shapes=[dma((5,))],
    )(*results)


def solution(mesh):
    return jax.shard_map(
        per_device,
        mesh=mesh,
        in_specs=(
            P(("gr", "sp"), "tp"),
            P(None, "tp"),
            P(None, "tp"),
            P(),
            P(),
            P(),
            P(None, "tp"),
            P(None, "tp"),
            P("gr", "tp", None),
            P("gr", "tp", None),
            P("gr"),
            P("tp", None),
        ),
        out_specs=(P("gr", None, "tp", "sp"), P("gr", "tp", None)),
        check_vma=False,
    )
```
